512 devices in a mesh: sp: 32 (over z, core), tp: 16 (over y, x).
Axes of the slice: x: 4, y: 4, z: 16, core: 2. Of those that a mesh axis runs over, the one named last changes fastest.
Arguments:
- moe_input: bfloat16 [5632, 2048], P('sp'), may hold values from -6 to 6
- cotangent: bfloat16 [5632, 2048], P('sp'), may hold values from -6 to 6
- route_ids: int32 [5632, 2], P('sp'), may hold values from 0 to 31, all different within a row; in each aligned block of 176 rows (0 to 175, 176 to 351, ...) at most 22 rows name the same one
- route_weights: float32 [5632, 2], P('sp'), may hold values from 0.25 to 1.5
- expert_gate: bfloat16 [32, 2048, 1024], P('sp', None, 'tp'), may hold values from -0.125 to 0.125
- expert_up: bfloat16 [32, 2048, 1024], P('sp', None, 'tp'), may hold values from -0.125 to 0.125
- expert_down: bfloat16 [32, 1024, 2048], P('sp', 'tp'), may hold values from -0.1875 to 0.1875
- out_proj: bfloat16 [2048, 2048], P('tp'), may hold values from -0.125 to 0.125
- gate_b: bfloat16 [5632, 2048], P('sp', 'tp'), may hold values from -6 to 6
- gate_c: bfloat16 [5632, 2048], P('sp', 'tp'), may hold values from -6 to 6
- conv_in: bfloat16 [5632, 2048], P('sp', 'tp'), may hold values from -6 to 6
- taps: float32 [3, 2048], P(None, 'tp'), may hold values from -4 to 4
Outputs:
- grad_expert_gate: float32 [32, 2048, 1024], P('sp', None, 'tp')
- grad_expert_up: float32 [32, 2048, 1024], P('sp', None, 'tp')
- grad_expert_down: float32 [32, 1024, 2048], P('sp', 'tp')
- grad_out_proj: float32 [2048, 2048], P('tp', 'sp')
- grad_gate_b: bfloat16 [5632, 2048], P('sp', 'tp')
- grad_gate_c: bfloat16 [5632, 2048], P('sp', 'tp')
- grad_conv_in: bfloat16 [5632, 2048], P('sp', 'tp')
The draws below stay inside these ranges and needn't reach their ends.
Inputs may be any that keep to these rules, and one draw needn't show every extreme that they name: `route_ids`: in the 176 rows of each index of sp, each row names 2 different experts, no expert is named by more than 22 rows, a bound that some block reaches.
All inputs are finite; a program needn't handle non-finite values.
Results may differ from the reference program's by a relative error of at most 0.033.
Values may be sent and summed in bfloat16 or wider, within the bound.
A program may use at most 64 MiB of HBM per device.

```python
import math
import jax
import jax.numpy as jnp
import numpy as np
from jax import lax

D = 2048
FF = 1024
TOPK = 2
TAPS = 3
TOK_SP = 176
TOKENS = 5632
EXPERTS = 32
CAP = 22
N_SP = 32
N_TP = 16


def raised(array, own_key, source, target, parts, factor):
    owner, partner = [(jnp.arange(array.shape[axis_at]) // (array.shape[axis_at] // parts)).reshape([-1 if axis == axis_at else 1 for axis in range(array.ndim)]) for axis_at in (source, target)]
    chosen = jax.random.permutation(own_key, parts)[partner]
    strong = (owner == chosen) | (owner == (partner + parts // 2) % parts)
    return jnp.where(strong, factor * array, array)


def block_scale(key, extent, cuts, low, top_value):
    def one(dim, parts):
        heights = jax.random.uniform(jax.random.fold_in(jax.random.fold_in(key, 6), dim), (parts,), jnp.float32, low / len(cuts), top_value / len(cuts))
        return jnp.repeat(jnp.exp(heights), extent[dim] // parts).reshape((-1,) + (1,) * (len(extent) - dim - 1))

    gain = one(*cuts[0])
    for cut in cuts[1:]:
        gain = gain * one(*cut)
    return gain


def shared_out(own_key, own, number, rows, count, top, reach, skew):
    sequence = jax.random.permutation(own_key, count)
    crowded, common = shares(count, rows * top, reach, skew, True), shares(count, rows * top, reach, skew, False)
    places = jnp.arange(count)

    def named(lengths, rotation):
        used = int((lengths > 0).sum())
        fixed = max(1, used // 4)
        passed = fixed + (places - fixed + rotation * (used - fixed)) % max(1, count - fixed)
        return jnp.zeros((count,), jnp.int32).at[sequence[jnp.where(places < fixed, places, passed)]].set(jnp.asarray(lengths, jnp.int32))

    lengths = jnp.where(number % 4 == 0, named(crowded, number // 4), named(common, number - number // 4 - 1))
    mixed = jax.random.permutation(jax.random.fold_in(own, 3), count)
    source_of, receiver = mixed[0:count // 2 * 2:2], mixed[1:count // 2 * 2:2]
    room = jnp.minimum(lengths[source_of] - 1, reach - lengths[receiver]) // 2
    room = jnp.where((source_of == sequence[0]) | (receiver == sequence[0]) | (lengths[receiver] == 0), 0, jnp.maximum(room, 0))
    passed = jax.random.randint(jax.random.fold_in(own, 4), (count // 2,), 0, 1 << 20) % (room + 1)
    lengths = lengths.at[source_of].add(-passed).at[receiver].add(passed)
    items = jnp.searchsorted(jnp.cumsum(lengths), jnp.arange(rows * top), side="right").astype(jnp.int32)
    grid = items.reshape(top, rows).T
    grid = grid[jax.random.permutation(jax.random.fold_in(own, 1), rows)]
    rotation = jax.random.randint(jax.random.fold_in(own, 2), (rows, 1), 0, top)
    return jnp.take_along_axis(grid, (jnp.arange(top)[None, :] + rotation) % top, axis=1)


def shares(amount, total, limit, slope, full):
    portions = [(1 << 20) // math.isqrt(standing ** slope) + 1 for standing in range(1, amount + 1)]
    largest = limit if full else min(limit, max(-(-total // amount), total * portions[0] // sum(portions)))
    least = 1 if total - largest >= amount - 1 else 0
    counts, rest = [largest] + [least] * (amount - 1), total - largest - least * (amount - 1)
    while rest > 0:
        candidates = [i for i in range(1, amount) if counts[i] < largest] or [i for i in range(1, amount) if counts[i] < limit]
        pool, left = sum([portions[i] for i in candidates]), rest
        for i in candidates:
            extra = min(limit - counts[i], max(1, left * portions[i] // pool), rest)
            counts[i] = counts[i] + extra
            rest = rest - extra
    return np.array(counts)


def scatter_about(own_key, extent, deviation, bound, shards=(), kind=jnp.bfloat16):
    entries = deviation * jax.random.normal(own_key, extent, jnp.float32)
    if shards:
        entries = entries * block_scale(own_key, extent, shards, -0.22, 0.18)
    return jnp.clip(entries, -bound, bound).astype(kind)


def bell_draw_with(rng, extent, spread, bound, split, heavy, held_as=jnp.bfloat16):
    entries = spread * jax.random.normal(rng, extent, jnp.float32)
    if split:
        entries = entries * block_scale(rng, extent, split, -0.22, 0.18)
    return jnp.clip(raised(entries, jax.random.fold_in(rng, 3), *heavy), -bound, bound).astype(held_as)


def setup_inputs(seed: int = 0) -> dict:
    streams_of = jax.random.split(jax.random.key(seed), 13)
    moe_input = scatter_about(streams_of[0], (TOKENS, D), 1.0, 6.0, ((0, 32),))
    cotangent = bell_draw_with(streams_of[1], (TOKENS, D), 1.0, 6.0, ((0, 32),), (0, 1, 32, 2.75))
    route_ids_keys = jax.random.split(jax.random.fold_in(streams_of[2], 1), TOKENS // TOK_SP)
    route_ids_turns = jax.random.permutation(jax.random.fold_in(streams_of[2], 3), TOKENS // TOK_SP)
    route_ids = jax.vmap(lambda own, number: shared_out(jax.random.fold_in(streams_of[2], 2), own, number, TOK_SP, EXPERTS, TOPK, CAP, 2))(route_ids_keys, route_ids_turns).reshape((TOKENS, TOPK))
    route_weights = jnp.clip(0.25 + 1.25 * jax.random.uniform(streams_of[3], (TOKENS, TOPK), jnp.float32) ** block_scale(streams_of[3], (TOKENS, TOPK), ((0, 32),), -0.2, 0.2), 0.25, 1.5)
    expert_gate = scatter_about(streams_of[4], (EXPERTS, D, FF), D ** -0.5, 0.125, ((0, 32), (2, 16)))
    expert_up = scatter_about(streams_of[5], (EXPERTS, D, FF), D ** -0.5, 0.125, ((0, 32), (2, 16)))
    expert_down = scatter_about(streams_of[6], (EXPERTS, FF, D), FF ** -0.5, 0.1875, ((0, 32), (1, 16)))
    out_proj = scatter_about(streams_of[7], (D, D), D ** -0.5, 0.125, ((0, 16),))
    gate_b = scatter_about(streams_of[8], (TOKENS, D), 1.0, 6.0, ((0, 32), (1, 16)))
    gate_c = scatter_about(streams_of[9], (TOKENS, D), 1.0, 6.0, ((0, 32), (1, 16)))
    conv_in = scatter_about(streams_of[10], (TOKENS, D), 1.0, 6.0, ((0, 32), (1, 16)))
    taps = scatter_about(streams_of[11], (TAPS, D), 0.6, 4.0, ((1, 16),), jnp.float32)
    return {"moe_input": moe_input, "cotangent": cotangent, "route_ids": route_ids, "route_weights": route_weights, "expert_gate": expert_gate, "expert_up": expert_up, "expert_down": expert_down, "out_proj": out_proj, "gate_b": gate_b, "gate_c": gate_c, "conv_in": conv_in, "taps": taps}


def slot_table(routes, experts, capacity):
    flattened = routes.reshape(-1)
    onehot = (flattened[:, None] == jnp.arange(experts, dtype=jnp.int32)[None, :]).astype(jnp.int32)
    earlier = jnp.cumsum(onehot, axis=0) - onehot
    return flattened * capacity + jnp.sum(earlier * onehot, axis=1)


def expert_backward(packed):
    rows_x, rows_s, weight_gate, weight_up, weight_down = packed
    pre_gate = jnp.dot(rows_x, weight_gate, preferred_element_type=jnp.float32)
    pre_up = jnp.dot(rows_x, weight_up, preferred_element_type=jnp.float32)
    sigma = jax.nn.sigmoid(pre_gate)
    active = pre_gate * sigma
    hidden = (active * pre_up).astype(jnp.bfloat16)
    back = jnp.dot(rows_s, weight_down.T, preferred_element_type=jnp.float32)
    grad_pre_gate = (back * pre_up * sigma * (1.0 + pre_gate * (1.0 - sigma))).astype(jnp.bfloat16)
    grad_pre_up = (back * active).astype(jnp.bfloat16)
    grad_down = jnp.dot(hidden.T, rows_s, preferred_element_type=jnp.float32)
    grad_gate = jnp.dot(rows_x.T, grad_pre_gate, preferred_element_type=jnp.float32)
    grad_up = jnp.dot(rows_x.T, grad_pre_up, preferred_element_type=jnp.float32)
    piece = FF // N_TP
    split_gate = grad_pre_gate.astype(jnp.float32).reshape(-1, N_TP, piece)
    split_up = grad_pre_up.astype(jnp.float32).reshape(-1, N_TP, piece)
    wide_gate = weight_gate.astype(jnp.float32).reshape(D, N_TP, piece)
    wide_up = weight_up.astype(jnp.float32).reshape(D, N_TP, piece)
    partial_value = jnp.einsum('sti,dti->tsd', split_gate, wide_gate) + jnp.einsum('sti,dti->tsd', split_up, wide_up)
    slot_grad = jnp.sum(partial_value.astype(jnp.bfloat16).astype(jnp.float32), axis=0).astype(jnp.bfloat16)
    return grad_gate, grad_up, grad_down, slot_grad


def reference(moe_input, cotangent, route_ids, route_weights, expert_gate, expert_up, expert_down, out_proj, gate_b, gate_c, conv_in, taps):
    assigned = TOKENS * TOPK
    blocks = route_ids.reshape(N_SP, TOK_SP * TOPK)
    local = jax.vmap(lambda ids: slot_table(ids, EXPERTS, CAP))(blocks)
    source = jnp.arange(N_SP, dtype=jnp.int32)[:, None]
    global_slot = (blocks * (N_SP * CAP) + source * CAP + (local - blocks * CAP)).reshape(-1).astype(jnp.int32)
    owner = jnp.full((EXPERTS * N_SP * CAP,), assigned, jnp.int32).at[global_slot].set(jnp.arange(assigned, dtype=jnp.int32))
    token_owner = jnp.where(owner < assigned, owner // TOPK, TOKENS).astype(jnp.int32)
    scaled = (route_weights[:, :, None] * cotangent[:, None, :].astype(jnp.float32)).astype(jnp.bfloat16).reshape(assigned, D)
    padded_x = jnp.concatenate([moe_input, jnp.zeros((1, D), jnp.bfloat16)], axis=0)
    padded_s = jnp.concatenate([scaled, jnp.zeros((1, D), jnp.bfloat16)], axis=0)
    slots_x = padded_x[token_owner].reshape(EXPERTS, N_SP * CAP, D)
    slots_s = padded_s[owner].reshape(EXPERTS, N_SP * CAP, D)
    grad_gate, grad_up, grad_down, slot_grad = lax.map(expert_backward, (slots_x, slots_s, expert_gate, expert_up, expert_down))
    slot_rows = slot_grad.reshape(-1, D)
    moe_rows = slot_rows[global_slot].astype(jnp.float32).reshape(TOKENS, TOPK, D).sum(axis=1)
    stream_grad = (cotangent.astype(jnp.float32) + moe_rows).astype(jnp.bfloat16)
    mixed = gate_c.astype(jnp.float32) * conv_in.astype(jnp.float32)
    mixed_pad = jnp.pad(mixed, ((2, 0), (0, 0)))
    conv = taps[2] * mixed + taps[1] * mixed_pad[1:-1] + taps[0] * mixed_pad[:-2]
    merged = (gate_b.astype(jnp.float32) * conv).astype(jnp.bfloat16)
    grad_merged = jnp.dot(stream_grad, out_proj.T, preferred_element_type=jnp.float32)
    grad_gate_b = (grad_merged * conv).astype(jnp.bfloat16)
    grad_conv = grad_merged * gate_b.astype(jnp.float32)
    grad_pad = jnp.pad(grad_conv, ((0, 2), (0, 0)))
    grad_mixed = taps[2] * grad_conv + taps[1] * grad_pad[1:-1] + taps[0] * grad_pad[2:]
    grad_gate_c = (grad_mixed * conv_in.astype(jnp.float32)).astype(jnp.bfloat16)
    grad_conv_in = (grad_mixed * gate_c.astype(jnp.float32)).astype(jnp.bfloat16)
    grad_out_proj = jnp.dot(merged.T, stream_grad, preferred_element_type=jnp.float32)
    return (grad_gate, grad_up, grad_down, grad_out_proj, grad_gate_b, grad_gate_c, grad_conv_in)
```

```python
import functools

import jax
import jax.numpy as jnp
from jax import lax
from jax.experimental import pallas as pl
from jax.experimental.pallas import tpu as pltpu
from jax.sharding import PartitionSpec as P

MESH = pl.DeviceIdType.MESH
BF = jnp.bfloat16
F32 = jnp.float32
NX = 4
NY = 4
W = 128


def dot(a, b, ca, cb):
    return lax.dot_general(a, b, (((ca,), (cb,)), ((), ())), preferred_element_type=F32)


def kernel(
    ns, cp,
    ids_ref, wts_ref, x_hbm, c_hbm, wg_hbm, wu_hbm, wd_hbm, op_hbm, gb_ref, gc_ref, ci_ref, taps_ref,
    gg_out, gu_out, gd_out, gp_out, ggb_out, ggc_out, gci_out,
    xcol, ccol, opv, disp, gx, wx, rows, preb, rs1, rs2, act, slotp, xr1, xr2, ret, retr, pt, st,
    gs, gr, mhs, mh, ghs, gh, gpo, gpp, pr, gq, fr,
    loc_sem, bsem_w, wsem_s, wsem_r, d_s, d_r, gx_s, gx_r, gxf_s, gxf_r, y_s, y_r, a_s, a_r, af_s, af_r,
    xs_s, xs_r, r_s, r_r, st_s, st_r, gw_s, gw_r, h_s, h_r, p_s, p_r, f_s, f_r,
):
    me = lax.axis_index("sp")
    tp = lax.axis_index("tp")
    ym = lax.div(tp, NX)
    xm = lax.rem(tp, NX)
    core = lax.rem(me, 2)
    zm = lax.div(me, 2)
    nz = ns // 2
    t = ids_ref.shape[1]
    n_rows = ns * cp
    nq = ns // 4
    qr = nq * cp
    qh = qr // 2
    half = n_rows // 2

    def xdev(d):
        return ym * NX + lax.rem(xm + d, NX)

    def ydev(d):
        return lax.rem(ym + d, NY) * NX + xm

    def rc(src, dst, ss, rs, **where):
        return pltpu.make_async_remote_copy(
            src_ref=src, dst_ref=dst, send_sem=ss, recv_sem=rs, device_id=where, device_id_type=MESH
        )

    barrier = pltpu.get_barrier_semaphore()

    @pl.loop(1, ns)
    def _(d):
        pl.semaphore_signal(barrier, inc=1, device_id={"sp": lax.rem(me + d, ns)}, device_id_type=MESH)

    @pl.loop(1, NX * NY)
    def _(d):
        pl.semaphore_signal(barrier, inc=1, device_id={"tp": lax.rem(tp + d, NX * NY)}, device_id_type=MESH)

    cols = pl.ds(pl.multiple_of(tp * W, W), W)
    yb = 4 * W
    load_x = pltpu.make_async_copy(x_hbm.at[:, cols], xcol, loc_sem.at[0])
    load_c = pltpu.make_async_copy(c_hbm.at[:, cols], ccol, loc_sem.at[1])
    load_o = pltpu.make_async_copy(op_hbm, opv, loc_sem.at[2])
    mats = (wg_hbm, wu_hbm, wd_hbm)
    ycols = pl.ds(pl.multiple_of(ym * yb, yb), yb)
    load_w = [pltpu.make_async_copy(mats[m].at[:, ycols], wx.at[ym, m], bsem_w.at[m]) for m in range(3)]
    load_x.start()
    load_c.start()
    for m in range(3):
        load_w[m].start()
    load_o.start()

    id0 = ids_ref[0:1, :]
    id1 = ids_ref[1:2, :]
    eio = lax.broadcasted_iota(jnp.int32, (ns, t), 0)
    oh0 = (eio == id0).astype(F32)
    oh1 = (eio == id1).astype(F32)
    before = (lax.broadcasted_iota(jnp.int32, (t, t), 0) < lax.broadcasted_iota(jnp.int32, (t, t), 1)).astype(F32).astype(BF)
    cum = dot((oh0 + oh1).astype(BF), before, 1, 0)
    slot0 = id0 * cp + jnp.sum(oh0 * cum, axis=0, keepdims=True).astype(jnp.int32)
    slot1 = id1 * cp + jnp.sum(oh1 * cum, axis=0, keepdims=True).astype(jnp.int32)
    rio = lax.broadcasted_iota(jnp.int32, (n_rows, t), 0)
    p0 = rio == slot0
    p1 = rio == slot1
    pmat = jnp.where(p0 | p1, 1.0, 0.0)
    wslot = jnp.sum(jnp.where(p0, wts_ref[0:1, :], jnp.where(p1, wts_ref[1:2, :], 0.0)), axis=1, keepdims=True)
    pb = pmat.astype(BF)
    load_x.wait()
    load_c.wait()
    picked = dot(pb, jnp.concatenate([xcol[...], ccol[...]], axis=1), 1, 0)
    disp[:, 0] = picked[:, :W].reshape(ns, cp, W).astype(BF)
    disp[:, 1] = (wslot * picked[:, W:]).reshape(ns, cp, W).astype(BF)

    mixed = gc_ref[...].astype(F32) * ci_ref[...].astype(F32)
    mhs[...] = mixed[t - 8 :, :]

    pl.semaphore_wait(barrier, ns - 1 + NX * NY - 1)

    def dispatch(d):
        i = lax.rem(me + d, ns)
        return rc(disp.at[i], gx.at[xm, me], d_s.at[i], d_r.at[me], sp=i)

    def arrival(i):
        return rc(disp.at[i], gx.at[xm, i], d_s.at[i], d_r.at[i], sp=i)

    @pl.loop(1, ns)
    def _(d):
        dispatch(d).start()

    halo_m = rc(mhs, mh, h_s.at[0], h_r.at[0], sp=lax.rem(me + 1, ns))
    halo_m.start()

    def wcopy(d, m, dst):
        block = pl.ds(pl.multiple_of(lax.rem(ym + d, NY) * yb, yb), yb)
        return rc(mats[m].at[:, block], wx.at[dst, m], wsem_s.at[d - 1, m], wsem_r.at[d - 1, m], tp=ydev(d))

    def wsend(d, m):
        return wcopy(d, m, ym)

    def wrecv(d, m):
        return wcopy(d, m, lax.rem(ym - d + NY, NY))

    for d in (1, 3, 2):
        for m in range(3):
            wsend(d, m).start()

    gx[xm, me] = disp[me]

    pt[...] = pmat.T.astype(BF)

    def gsend(q, s):
        part = pl.ds(q * nq, nq)
        d = 1 if s == 0 else NX - 1
        return rc(gx.at[xm, part], gx.at[xm, part], gx_s.at[s, q], gx_r.at[s, q], tp=xdev(d))

    def grecv(q, s):
        part = pl.ds(q * nq, nq)
        d = NX - 1 if s == 0 else 1
        src = lax.rem(xm + d, NX)
        return rc(gx.at[xm, part], gx.at[src, part], gx_s.at[s, q], gx_r.at[s, q], tp=xdev(d))

    def gforward(q):
        part = pl.ds(q * nq, nq)
        s = 0 if q < 2 else 1
        src = lax.rem(xm + (NX - 1 if s == 0 else 1), NX)
        d = 1 if s == 0 else NX - 1
        return rc(gx.at[src, part], gx.at[src, part], gxf_s.at[q], gxf_r.at[q], tp=xdev(d))

    def gfar(q):
        part = pl.ds(q * nq, nq)
        far = lax.rem(xm + 2, NX)
        return rc(gx.at[far, part], gx.at[far, part], gxf_s.at[q], gxf_r.at[q], tp=xdev(2))

    for q in range(4):
        @pl.loop(0, nq)
        def _(k, q=q):
            i = q * nq + k

            @pl.when(i != me)
            def _():
                arrival(i).wait_recv()

        gsend(q, 0).start()
        gsend(q, 1).start()

    for q in range(4):
        if q < 2:
            grecv(q, 0).wait_recv()
            gforward(q).start()
            grecv(q, 1).wait_recv()
        else:
            grecv(q, 1).wait_recv()
            gforward(q).start()
            grecv(q, 0).wait_recv()

    for m in range(3):
        load_w[m].wait()
        for d in (1, 2, 3):
            wrecv(d, m).wait_recv()

    for q in range(4):
        gfar(q).wait_recv()
    w3 = [jnp.concatenate([wx[yy, m] for yy in range(NY)], axis=0) for m in range(3)]

    @pl.loop(0, 4)
    def _(q):
        for s in range(2):
            blocks = [gx[xx, pl.ds(q * nq, nq), s].astype(F32).reshape(qr, W) for xx in range(NX)]
            rows[s, q] = jnp.concatenate(blocks, axis=1).astype(BF)
        for m in range(3):
            preb[q, :, m * 2 * W : (m + 1) * 2 * W] = dot(rows[1 if m == 2 else 0, q], w3[m], 1, 1).astype(BF)

    low, high = pl.ds(0, qh), pl.ds(qh, qh)
    up, down, far = lax.rem(ym + 1, NY), lax.rem(ym + 3, NY), lax.rem(ym + 2, NY)
    y_far_up = rc(preb.at[far, low], rs1.at[0], y_s.at[0], y_r.at[0], tp=ydev(1))
    y_far_down = rc(preb.at[far, high], rs1.at[1], y_s.at[1], y_r.at[1], tp=ydev(3))
    y_up_b = rc(preb.at[up, high], rs2.at[0, high], y_s.at[2], y_r.at[2], tp=ydev(1))
    y_down_a = rc(preb.at[down, low], rs2.at[1, low], y_s.at[3], y_r.at[3], tp=ydev(3))
    y_up_a = rc(preb.at[up, low], rs2.at[0, low], y_s.at[4], y_r.at[4], tp=ydev(1))
    y_down_b = rc(preb.at[down, high], rs2.at[1, high], y_s.at[5], y_r.at[5], tp=ydev(3))
    y_far_up.start()
    y_far_down.start()
    y_up_b.start()
    y_down_a.start()
    y_far_up.wait_recv()
    preb[up, low] = (preb[up, low].astype(F32) + rs1[0].astype(F32)).astype(BF)
    y_up_a.start()
    y_far_down.wait_recv()
    preb[down, high] = (preb[down, high].astype(F32) + rs1[1].astype(F32)).astype(BF)
    y_down_b.start()
    y_up_b.wait_recv()
    y_down_a.wait_recv()
    y_up_a.wait_recv()
    y_down_b.wait_recv()
    u = 2 * W

    def total(m):
        c = slice(m * u, (m + 1) * u)
        return preb[ym, :, c].astype(F32) + rs2[0, :, c].astype(F32) + rs2[1, :, c].astype(F32)

    pre_gate = total(0)
    pre_up = total(1)
    back = total(2)
    sigma = jax.nn.sigmoid(pre_gate)
    active = pre_gate * sigma
    act[ym, :, 0:u] = (back * pre_up * sigma * (1.0 + pre_gate * (1.0 - sigma))).astype(BF)
    act[ym, :, u : 2 * u] = (back * active).astype(BF)
    act[ym, :, 2 * u :] = (active * pre_up).astype(BF)

    a_up = rc(act.at[ym], act.at[ym], a_s.at[0], a_r.at[0], tp=ydev(1))
    a_down = rc(act.at[ym], act.at[ym], a_s.at[1], a_r.at[1], tp=ydev(3))
    a_up.start()
    a_down.start()
    rc(act.at[ym], act.at[down], a_s.at[0], a_r.at[0], tp=ydev(3)).wait_recv()
    af_up = rc(act.at[down, low], act.at[down, low], af_s.at[0], af_r.at[0], tp=ydev(1))
    af_up.start()
    rc(act.at[ym], act.at[up], a_s.at[1], a_r.at[1], tp=ydev(1)).wait_recv()
    af_down = rc(act.at[up, high], act.at[up, high], af_s.at[1], af_r.at[1], tp=ydev(3))
    af_down.start()
    rc(act.at[far, low], act.at[far, low], af_s.at[0], af_r.at[0], tp=ydev(2)).wait_recv()
    rc(act.at[far, high], act.at[far, high], af_s.at[1], af_r.at[1], tp=ydev(2)).wait_recv()

    @pl.loop(0, 4)
    def _(q):
        part = dot(act[q, :, 0:u], w3[0], 1, 0) + dot(act[q, :, u : 2 * u], w3[1], 1, 0)
        for xx in range(NX):
            slotp[xx, pl.ds(pl.multiple_of(q * qr, qr), qr), :] = part[:, xx * W : (xx + 1) * W].astype(BF)

    lo, hi = pl.ds(0, half), pl.ds(half, half)
    xr, xl, xf = lax.rem(xm + 1, NX), lax.rem(xm + 3, NX), lax.rem(xm + 2, NX)
    x_far_r = rc(slotp.at[xf, lo], xr1.at[0], xs_s.at[0], xs_r.at[0], tp=xdev(1))
    x_far_l = rc(slotp.at[xf, hi], xr1.at[1], xs_s.at[1], xs_r.at[1], tp=xdev(3))
    x_r_b = rc(slotp.at[xr, hi], xr2.at[0, hi], xs_s.at[2], xs_r.at[2], tp=xdev(1))
    x_l_a = rc(slotp.at[xl, lo], xr2.at[1, lo], xs_s.at[3], xs_r.at[3], tp=xdev(3))
    x_r_a = rc(slotp.at[xr, lo], xr2.at[0, lo], xs_s.at[4], xs_r.at[4], tp=xdev(1))
    x_l_b = rc(slotp.at[xl, hi], xr2.at[1, hi], xs_s.at[5], xs_r.at[5], tp=xdev(3))
    x_far_r.start()
    x_far_l.start()
    x_r_b.start()
    x_l_a.start()
    x_far_r.wait_recv()
    slotp[xr, lo] = (slotp[xr, lo].astype(F32) + xr1[0].astype(F32)).astype(BF)
    x_r_a.start()
    x_far_l.wait_recv()
    slotp[xl, hi] = (slotp[xl, hi].astype(F32) + xr1[1].astype(F32)).astype(BF)
    x_l_b.start()

    for m in range(3):
        left = act[:, :, m * u : (m + 1) * u].reshape(n_rows, u)
        right = rows[1 if m == 2 else 0].reshape(n_rows, yb)
        gs[:, m] = dot(left, right, 0, 0).reshape(NY, 64, yb).astype(BF)

    def gwsend(d):
        return rc(gs.at[lax.rem(ym + d, NY)], gr.at[ym], gw_s.at[d - 1], gw_r.at[d - 1], tp=ydev(d))

    def gwrecv(d):
        return rc(gs.at[ym], gr.at[lax.rem(ym - d + NY, NY)], gw_s.at[d - 1], gw_r.at[d - 1], tp=ydev(d))

    x_r_b.wait_recv()
    x_l_a.wait_recv()
    x_r_a.wait_recv()
    x_l_b.wait_recv()
    slot = slotp[xm].astype(F32) + xr2[0].astype(F32) + xr2[1].astype(F32)
    ret[...] = slot.reshape(ns, cp, W).astype(BF)

    @pl.loop(1, ns)
    def _(d):
        i = lax.rem(me + d, ns)
        rc(ret.at[i], retr.at[me], r_s.at[i], r_r.at[me], sp=i).start()

    for d in (1, 3, 2):
        gwsend(d).start()
    retr[me] = ret[me]
    gr[ym] = gs[ym]

    halo_m.wait_recv()
    prev = jnp.where(me == 0, 0.0, mh[...])
    ext = jnp.concatenate([prev, mixed], axis=0)
    tap = taps_ref[...]
    conv = tap[2:3] * mixed + tap[1:2] * ext[7 : 7 + t] + tap[0:1] * ext[6 : 6 + t]
    merged = (gb_ref[...].astype(F32) * conv).astype(BF)

    @pl.loop(1, ns)
    def _(d):
        i = lax.rem(me + d, ns)
        rc(ret.at[i], retr.at[i], r_s.at[i], r_r.at[i], sp=i).wait_recv()

    back_rows = retr[...].astype(F32).reshape(n_rows, W).astype(BF)
    grad_cols = ccol[...].astype(F32) + dot(pt[...], back_rows, 1, 0)
    st[tp] = grad_cols.astype(BF)

    def stsend(d):
        return rc(st.at[tp], st.at[tp], st_s.at[d - 1], st_r.at[d - 1], tp=lax.rem(tp + d, NX * NY))

    def strecv(d):
        src = lax.rem(tp - d + NX * NY, NX * NY)
        return rc(st.at[tp], st.at[src], st_s.at[d - 1], st_r.at[d - 1], tp=src)

    @pl.loop(1, NX * NY)
    def _(d):
        stsend(d).start()

    for d in (1, 2, 3):
        gwrecv(d).wait_recv()
    for m, out in enumerate((gg_out, gu_out, gd_out)):
        for yy in range(NY):
            out[:, yy * yb : (yy + 1) * yb] = gr[yy, m].astype(F32)
    load_o.wait()

    @pl.loop(1, NX * NY)
    def _(d):
        strecv(d).wait_recv()

    stream = jnp.concatenate([st[j] for j in range(NX * NY)], axis=1)
    grad_merged = dot(stream, opv[...], 1, 1)
    grad_conv = grad_merged * gb_ref[...].astype(F32)
    ghs[...] = grad_conv[0:8, :]
    halo_g = rc(ghs, gh, h_s.at[1], h_r.at[1], sp=lax.rem(me + ns - 1, ns))
    halo_g.start()

    proj = dot(stream, merged, 0, 0).reshape(NX * NY, 2, 64, W)
    proj0 = proj[:, 0]
    proj1 = proj[:, 1]
    gpo[...] = jnp.where(core == 0, proj0, proj1)
    gpp[...] = jnp.where(core == 0, proj1, proj0).astype(BF)
    pair = rc(gpp, pr, p_s.at[0], p_r.at[0], sp=zm * 2 + 1 - core)
    pair.start()
    ggb_out[...] = (grad_merged * conv).astype(BF)
    pair.wait_recv()
    gpo[...] = gpo[...] + pr[...].astype(F32)
    gq[...] = gpo[...].astype(BF)

    @pl.loop(1, nz)
    def _(d):
        z = lax.rem(zm + d, nz)
        rc(gq.at[z], fr.at[zm], f_s.at[z], f_r.at[zm], sp=z * 2 + core).start()

    halo_g.wait_recv()
    following = jnp.where(me == ns - 1, 0.0, gh[...])
    extg = jnp.concatenate([grad_conv, following], axis=0)
    grad_mixed = tap[2:3] * grad_conv + tap[1:2] * extg[1 : 1 + t] + tap[0:1] * extg[2 : 2 + t]
    ggc_out[...] = (grad_mixed * ci_ref[...].astype(F32)).astype(BF)
    gci_out[...] = (grad_mixed * gc_ref[...].astype(F32)).astype(BF)

    @pl.loop(1, ns)
    def _(d):
        dispatch(d).wait_send()
        i = lax.rem(me + d, ns)
        rc(ret.at[i], retr.at[me], r_s.at[i], r_r.at[me], sp=i).wait_send()

    halo_m.wait_send()
    halo_g.wait_send()
    for d in (1, 2, 3):
        for m in range(3):
            wsend(d, m).wait_send()
        gwsend(d).wait_send()
    for q in range(4):
        gsend(q, 0).wait_send()
        gsend(q, 1).wait_send()
        gforward(q).wait_send()
    for c in (y_far_up, y_far_down, y_up_b, y_down_a, y_up_a, y_down_b, a_up, a_down, af_up, af_down):
        c.wait_send()
    for c in (x_far_r, x_far_l, x_r_b, x_l_a, x_r_a, x_l_b, pair):
        c.wait_send()

    @pl.loop(1, NX * NY)
    def _(d):
        stsend(d).wait_send()

    @pl.loop(1, nz)
    def _(d):
        z = lax.rem(zm + d, nz)
        rc(gq.at[z], fr.at[z], f_s.at[z], f_r.at[z], sp=z * 2 + core).wait()

    fr[zm] = gq[zm]
    gp_out[...] = jnp.sum(fr[...].astype(F32), axis=0)


def on_device(
    moe_input, cotangent, route_ids, route_weights, expert_gate, expert_up, expert_down,
    out_proj, gate_b, gate_c, conv_in, taps,
):
    ns = lax.axis_size("sp")
    t, model = moe_input.shape
    cap = 2 * t * route_ids.shape[1] // ns
    cp = -(-cap // 8) * 8
    n_rows = ns * cp
    qr = n_rows // 4
    yb = model // NY
    tpn = NX * NY
    units = expert_gate.shape[2]
    sds = jax.ShapeDtypeStruct
    vmem = pl.BlockSpec(memory_space=pltpu.VMEM)
    anym = pl.BlockSpec(memory_space=pl.ANY)
    dma = pltpu.SemaphoreType.DMA
    V = pltpu.VMEM
    scratch = [
        V((t, W), BF), V((t, W), BF), V((W, model), BF), V((ns, 2, cp, W), BF), V((NX, ns, 2, cp, W), BF),
        V((NY, 3, units, yb), BF), V((2, 4, qr, yb), BF), V((4, qr, 6 * W), BF), V((2, qr // 2, 6 * W), BF),
        V((2, qr, 6 * W), BF), V((4, qr, 6 * W), BF), V((NX, n_rows, W), BF), V((2, n_rows // 2, W), BF),
        V((2, n_rows, W), BF), V((ns, cp, W), BF), V((ns, cp, W), BF), V((t, n_rows), BF), V((tpn, t, W), BF),
        V((NY, 3, units, yb), BF), V((NY, 3, units, yb), BF), V((8, W), F32), V((8, W), F32), V((8, W), F32), V((8, W), F32),
        V((tpn, 64, W), F32), V((tpn, 64, W), BF), V((tpn, 64, W), BF), V((tpn, 64, W), BF), V((tpn, 64, W), BF),
        dma((3,)), dma((3,)), dma((3, 3)), dma((3, 3)), dma((ns,)), dma((ns,)), dma((2, 4)), dma((2, 4)), dma((4,)), dma((4,)),
        dma((6,)), dma((6,)), dma((2,)), dma((2,)), dma((2,)), dma((2,)),
        dma((6,)), dma((6,)), dma((ns,)), dma((ns,)), dma((tpn - 1,)), dma((tpn - 1,)), dma((3,)), dma((3,)), dma((2,)), dma((2,)),
        dma((1,)), dma((1,)), dma((ns // 2,)), dma((ns // 2,)),
    ]
    outs = pl.pallas_call(
        functools.partial(kernel, ns, cp),
        out_shape=(
            sds((units, model), F32), sds((units, model), F32), sds((units, model), F32), sds((64, W), F32),
            sds((t, W), BF), sds((t, W), BF), sds((t, W), BF),
        ),
        in_specs=[vmem, vmem] + [anym] * 6 + [vmem] * 4,
        out_specs=[vmem] * 7,
        scratch_shapes=scratch,
        compiler_params=pltpu.CompilerParams(collective_id=0, has_side_effects=True, vmem_limit_bytes=56 * 2**20),
    )(
        route_ids.T, route_weights.T, moe_input, cotangent, expert_gate[0].T, expert_up[0].T, expert_down[0],
        out_proj, gate_b, gate_c, conv_in, taps,
    )
    gg, gu, gd, gp, ggb, ggc, gci = outs
    return gg.T[None], gu.T[None], gd[None], gp.T, ggb, ggc, gci


def solution(mesh):
    row, cols = P("sp", None), P("sp", "tp")
    return jax.shard_map(
        on_device,
        mesh=mesh,
        in_specs=(
            row, row, row, row, P("sp", None, "tp"), P("sp", None, "tp"), P("sp", "tp", None), P("tp", None),
            cols, cols, cols, P(None, "tp"),
        ),
        out_specs=(
            P("sp", None, "tp"), P("sp", None, "tp"), P("sp", "tp", None), P("tp", "sp"), cols, cols, cols,
        ),
        check_vma=False,
    )
```

```python
import functools

import jax
import jax.numpy as jnp
from jax import lax
from jax.experimental import pallas as pl
from jax.experimental.pallas import tpu as pltpu
from jax.sharding import PartitionSpec as P

MESH = pl.DeviceIdType.MESH
BF = jnp.bfloat16
F32 = jnp.float32
NX = 4
NY = 4
W = 128


def dot(a, b, ca, cb):
    return lax.dot_general(a, b, (((ca,), (cb,)), ((), ())), preferred_element_type=F32)


CHUNKS = (16, 8, 8)
STARTS = tuple(sum(CHUNKS[:k]) for k in range(len(CHUNKS)))
NC = len(CHUNKS)
LAG = 1
ORDER = (0, 1, 3, 2)


def kernel(
    ns, cp,
    ids_hbm, wts_hbm, x_hbm, c_hbm, wg_hbm, wu_hbm, wd_hbm, op_hbm, gb_hbm, gc_hbm, ci_hbm, taps_hbm,
    gg_out, gu_out, gd_out, gp_out, ggb_out, ggc_out, gci_out,
    ids_ref, wts_ref, gb_ref, gc_ref, ci_ref, taps_ref,
    xcol, ccol, opv, disp, gx, wx, rows, preb, rs1, rs2, act, slotp, xr1, xr2, ret, retr, pt, st,
    gs, gr, mhs, mh, ghs, gh, gpo, gpp, pr, gq, fr,
    loc_sem, bsem_w, wsem_s, wsem_r, d_s, d_r, gx_s, gx_r, gxf_s, gxf_r, y_s, y_r, a_s, a_r, af_s, af_r,
    xs_s, xs_r, r_s, r_r, st_s, st_r, gw_s, gw_r, h_s, h_r, p_s, p_r, f_s, f_r,
):
    me = lax.axis_index("sp")
    tp = lax.axis_index("tp")
    ym = lax.div(tp, NX)
    xm = lax.rem(tp, NX)
    core = lax.rem(me, 2)
    zm = lax.div(me, 2)
    nz = ns // 2
    t = ids_ref.shape[1]
    n_rows = ns * cp
    u = 2 * W
    yb = 4 * W

    def xdev(d):
        return ym * NX + lax.rem(xm + d, NX)

    def ydev(d):
        return lax.rem(ym + d, NY) * NX + xm

    def rc(src, dst, ss, rs, **where):
        return pltpu.make_async_remote_copy(
            src_ref=src, dst_ref=dst, send_sem=ss, recv_sem=rs, device_id=where, device_id_type=MESH
        )

    def offset(k):
        return lax.div(k + 1, 2) * (2 * lax.rem(k, 2) - 1)

    sends = []

    def go(copy):
        copy.start()
        sends.append(copy)

    barrier = pltpu.get_barrier_semaphore()
    small = [
        pltpu.make_async_copy(src, dst, loc_sem.at[k])
        for k, (src, dst) in enumerate(
            (
                (ids_hbm, ids_ref), (wts_hbm, wts_ref), (gb_hbm, gb_ref), (gc_hbm, gc_ref), (ci_hbm, ci_ref),
                (taps_hbm, taps_ref),
            )
        )
    ]
    cols = pl.ds(pl.multiple_of(tp * W, W), W)
    load_x = pltpu.make_async_copy(x_hbm.at[:, cols], xcol, loc_sem.at[6])
    load_c = pltpu.make_async_copy(c_hbm.at[:, cols], ccol, loc_sem.at[7])
    load_o = pltpu.make_async_copy(op_hbm, opv, loc_sem.at[8])
    mats = (wg_hbm, wu_hbm, wd_hbm)
    ycols = pl.ds(pl.multiple_of(ym * yb, yb), yb)
    load_w = [pltpu.make_async_copy(mats[m].at[:, ycols], wx.at[ym, m], bsem_w.at[m]) for m in range(3)]
    small[0].start()
    small[1].start()
    load_x.start()
    load_c.start()

    @pl.loop(1, ns)
    def _(d):
        pl.semaphore_signal(barrier, inc=1, device_id={"sp": lax.rem(me + d, ns)}, device_id_type=MESH)

    @pl.loop(1, NX * NY)
    def _(d):
        pl.semaphore_signal(barrier, inc=1, device_id={"tp": lax.rem(tp + d, NX * NY)}, device_id_type=MESH)

    for copy in small[2:]:
        copy.start()
    for copy in load_w:
        copy.start()
    load_o.start()

    small[0].wait()
    small[1].wait()
    id0 = ids_ref[0:1, :]
    id1 = ids_ref[1:2, :]
    eio = lax.broadcasted_iota(jnp.int32, (ns, t), 0)
    oh0 = (eio == id0).astype(F32)
    oh1 = (eio == id1).astype(F32)
    before = (lax.broadcasted_iota(jnp.int32, (t, t), 0) < lax.broadcasted_iota(jnp.int32, (t, t), 1)).astype(F32).astype(BF)
    cum = dot((oh0 + oh1).astype(BF), before, 1, 0)
    slot0 = id0 * cp + jnp.sum(oh0 * cum, axis=0, keepdims=True).astype(jnp.int32)
    slot1 = id1 * cp + jnp.sum(oh1 * cum, axis=0, keepdims=True).astype(jnp.int32)
    rio = lax.broadcasted_iota(jnp.int32, (n_rows, t), 0)
    p0 = rio == slot0
    p1 = rio == slot1
    pmat = jnp.where(p0 | p1, 1.0, 0.0)
    wslot = jnp.sum(jnp.where(p0, wts_ref[0:1, :], jnp.where(p1, wts_ref[1:2, :], 0.0)), axis=1, keepdims=True)
    pb = pmat.astype(BF)
    load_x.wait()
    load_c.wait()
    picked = dot(pb, jnp.concatenate([xcol[...], ccol[...]], axis=1), 1, 0)
    disp[:, 0] = picked[:, :W].reshape(ns, cp, W).astype(BF)
    disp[:, 1] = (wslot * picked[:, W:]).reshape(ns, cp, W).astype(BF)

    for copy in small[2:]:
        copy.wait()
    mixed = gc_ref[...].astype(F32) * ci_ref[...].astype(F32)
    mhs[...] = mixed[t - 8 :, :]

    pl.semaphore_wait(barrier, ns - 1 + NX * NY - 1)

    def dispatch(j):
        k = lax.div(j, 2)
        i = lax.rem(zm - offset(k) + nz, nz) * 2 + lax.rem(j, 2)
        return rc(disp.at[i], gx.at[xm, 2 * k + core], d_s.at[j], d_r.at[2 * k + core], sp=i)

    def arrival(p):
        return rc(disp.at[p], gx.at[xm, p], d_s.at[p], d_r.at[p], sp=lax.rem(me + 1, ns))

    dispatch(1 - core).start()

    @pl.loop(2, ns)
    def _(j):
        dispatch(j).start()

    def wcopy(d, m, dst):
        block = pl.ds(pl.multiple_of(lax.rem(ym + d, NY) * yb, yb), yb)
        return rc(mats[m].at[:, block], wx.at[dst, m], wsem_s.at[d - 1, m], wsem_r.at[d - 1, m], tp=ydev(d))

    for d in (1, 3, 2):
        for m in range(3):
            go(wcopy(d, m, ym))

    halo_m = rc(mhs, mh, h_s.at[0], h_r.at[0], sp=lax.rem(me + 1, ns))
    go(halo_m)

    gx[xm, core] = disp[me]

    pt[...] = pmat.T.astype(BF)

    right, left, xfar = lax.rem(xm + 1, NX), lax.rem(xm + 3, NX), lax.rem(xm + 2, NX)
    up, down, yfar = lax.rem(ym + 1, NY), lax.rem(ym + 3, NY), lax.rem(ym + 2, NY)

    def wait_on(dst, ss, rs):
        rc(dst, dst, ss, rs, tp=xdev(1)).wait_recv()

    weights = []

    def stage_a(c):
        at, pc = STARTS[c], CHUNKS[c]
        if c == 0:
            arrival(1 - core).wait_recv()

        @pl.loop(2 if c == 0 else at, at + pc)
        def _(p):
            arrival(p).wait_recv()

        part = gx.at[xm, pl.ds(at, pc)]
        go(rc(part, part, gx_s.at[c, 0], gx_r.at[c, 0], tp=xdev(1)))
        go(rc(part, part, gx_s.at[c, 1], gx_r.at[c, 1], tp=xdev(3)))

    def stage_b(c):
        at, pc = STARTS[c], CHUNKS[c]
        wait_on(gx.at[left, pl.ds(at, pc)], gx_s.at[c, 0], gx_r.at[c, 0])
        part = gx.at[left, pl.ds(at, pc // 2)]
        go(rc(part, part, gxf_s.at[c, 0], gxf_r.at[c, 0], tp=xdev(1)))
        wait_on(gx.at[right, pl.ds(at, pc)], gx_s.at[c, 1], gx_r.at[c, 1])
        part = gx.at[right, pl.ds(at + pc // 2, pc // 2)]
        go(rc(part, part, gxf_s.at[c, 1], gxf_r.at[c, 1], tp=xdev(3)))

    def pieces(c):
        yq = CHUNKS[c] * cp // NY
        cut = -(-yq // 32) * 16
        cut = cut if c % 2 == 0 else yq - cut
        return pl.ds(0, cut), pl.ds(cut, yq - cut)

    def stage_c(c):
        at, pc = STARTS[c], CHUNKS[c]
        qr = pc * cp
        yq = qr // NY
        if c == 0:
            for m in range(3):
                load_w[m].wait()
                for d in (1, 2, 3):
                    wcopy(d, m, lax.rem(ym - d + NY, NY)).wait_recv()
            weights.extend(jnp.concatenate([wx[yy, m] for yy in range(NY)], axis=0) for m in range(3))
        wait_on(gx.at[xfar, pl.ds(at, pc // 2)], gxf_s.at[c, 0], gxf_r.at[c, 0])
        wait_on(gx.at[xfar, pl.ds(at + pc // 2, pc // 2)], gxf_s.at[c, 1], gxf_r.at[c, 1])
        for s in range(2):
            blocks = [gx[xx, at : at + pc, s].astype(F32).reshape(qr, W) for xx in range(NX)]
            rows[c][s] = jnp.concatenate(blocks, axis=1).astype(BF)
        for m in range(3):
            pre = dot(rows[c][1 if m == 2 else 0], weights[m], 1, 1)
            preb[c][:, :, m * u : (m + 1) * u] = pre.reshape(NY, yq, u).astype(BF)
        low, high = pieces(c)
        go(rc(preb[c].at[yfar, low], rs1[c].at[low], y_s.at[c, 0], y_r.at[c, 0], tp=ydev(1)))
        go(rc(preb[c].at[yfar, high], rs1[c].at[high], y_s.at[c, 1], y_r.at[c, 1], tp=ydev(3)))
        go(rc(preb[c].at[up, high], rs2[c].at[0, high], y_s.at[c, 2], y_r.at[c, 2], tp=ydev(1)))
        go(rc(preb[c].at[down, low], rs2[c].at[1, low], y_s.at[c, 3], y_r.at[c, 3], tp=ydev(3)))

    def stage_d(c):
        low, high = pieces(c)
        wait_on(rs1[c].at[low], y_s.at[c, 0], y_r.at[c, 0])
        preb[c][up, low] = (preb[c][up, low].astype(F32) + rs1[c][low].astype(F32)).astype(BF)
        go(rc(preb[c].at[up, low], rs2[c].at[0, low], y_s.at[c, 4], y_r.at[c, 4], tp=ydev(1)))
        wait_on(rs1[c].at[high], y_s.at[c, 1], y_r.at[c, 1])
        preb[c][down, high] = (preb[c][down, high].astype(F32) + rs1[c][high].astype(F32)).astype(BF)
        go(rc(preb[c].at[down, high], rs2[c].at[1, high], y_s.at[c, 5], y_r.at[c, 5], tp=ydev(3)))

    def stage_e(c):
        low, high = pieces(c)
        for k, (row, part) in enumerate(((0, high), (1, low), (0, low), (1, high))):
            wait_on(rs2[c].at[row, part], y_s.at[c, 2 + k], y_r.at[c, 2 + k])

        def total(m):
            q = slice(m * u, (m + 1) * u)
            return preb[c][ym, :, q].astype(F32) + rs2[c][0, :, q].astype(F32) + rs2[c][1, :, q].astype(F32)

        pre_gate = total(0)
        pre_up = total(1)
        back = total(2)
        sigma = jax.nn.sigmoid(pre_gate)
        active = pre_gate * sigma
        act[c][ym, :, 0:u] = (back * pre_up * sigma * (1.0 + pre_gate * (1.0 - sigma))).astype(BF)
        act[c][ym, :, u : 2 * u] = (back * active).astype(BF)
        act[c][ym, :, 2 * u :] = (active * pre_up).astype(BF)
        own = act[c].at[ym]
        go(rc(own, own, a_s.at[c, 0], a_r.at[c, 0], tp=ydev(1)))
        go(rc(own, own, a_s.at[c, 1], a_r.at[c, 1], tp=ydev(3)))

    def stage_f(c):
        low, high = pieces(c)
        wait_on(act[c].at[down], a_s.at[c, 0], a_r.at[c, 0])
        part = act[c].at[down, low]
        go(rc(part, part, af_s.at[c, 0], af_r.at[c, 0], tp=ydev(1)))
        wait_on(act[c].at[up], a_s.at[c, 1], a_r.at[c, 1])
        part = act[c].at[up, high]
        go(rc(part, part, af_s.at[c, 1], af_r.at[c, 1], tp=ydev(3)))

    def halves(c):
        xh = CHUNKS[c] * cp // 2
        return pl.ds(0, xh), pl.ds(xh, xh)

    def stage_g(c):
        qr = CHUNKS[c] * cp
        lo, hi = halves(c)
        low, high = pieces(c)
        wait_on(act[c].at[yfar, low], af_s.at[c, 0], af_r.at[c, 0])
        wait_on(act[c].at[yfar, high], af_s.at[c, 1], af_r.at[c, 1])
        part = dot(act[c][:, :, 0:u].reshape(qr, u), weights[0], 1, 0)
        part = part + dot(act[c][:, :, u : 2 * u].reshape(qr, u), weights[1], 1, 0)
        for xx in range(NX):
            slotp[c][xx] = part[:, xx * W : (xx + 1) * W].astype(BF)
        go(rc(slotp[c].at[xfar, lo], xr1[c].at[0], xs_s.at[c, 0], xs_r.at[c, 0], tp=xdev(1)))
        go(rc(slotp[c].at[xfar, hi], xr1[c].at[1], xs_s.at[c, 1], xs_r.at[c, 1], tp=xdev(3)))
        go(rc(slotp[c].at[right, hi], xr2[c].at[0, hi], xs_s.at[c, 2], xs_r.at[c, 2], tp=xdev(1)))
        go(rc(slotp[c].at[left, lo], xr2[c].at[1, lo], xs_s.at[c, 3], xs_r.at[c, 3], tp=xdev(3)))

    def stage_h(c):
        lo, hi = halves(c)
        wait_on(xr1[c].at[0], xs_s.at[c, 0], xs_r.at[c, 0])
        slotp[c][right, lo] = (slotp[c][right, lo].astype(F32) + xr1[c][0].astype(F32)).astype(BF)
        go(rc(slotp[c].at[right, lo], xr2[c].at[0, lo], xs_s.at[c, 4], xs_r.at[c, 4], tp=xdev(1)))
        wait_on(xr1[c].at[1], xs_s.at[c, 1], xs_r.at[c, 1])
        slotp[c][left, hi] = (slotp[c][left, hi].astype(F32) + xr1[c][1].astype(F32)).astype(BF)
        go(rc(slotp[c].at[left, hi], xr2[c].at[1, hi], xs_s.at[c, 5], xs_r.at[c, 5], tp=xdev(3)))

    def giveback(p):
        k = lax.div(p, 2)
        i = lax.rem(zm + offset(k) + nz, nz) * 2 + lax.rem(p, 2)
        return rc(ret.at[p], retr.at[me], r_s.at[p], r_r.at[me], sp=i)

    def stage_i(c):
        at, pc = STARTS[c], CHUNKS[c]
        lo, hi = halves(c)
        for k, (row, part) in enumerate(((0, hi), (1, lo), (0, lo), (1, hi))):
            wait_on(xr2[c].at[row, part], xs_s.at[c, 2 + k], xs_r.at[c, 2 + k])
        slot = slotp[c][xm].astype(F32) + xr2[c][0].astype(F32) + xr2[c][1].astype(F32)
        ret[at : at + pc] = slot.reshape(pc, cp, W).astype(BF)
        if c == 0:
            giveback(1 - core).start()
            retr[me] = ret[core]

        @pl.loop(2 if c == 0 else at, at + pc)
        def _(p):
            giveback(p).start()

    def gwcopy(d, dst):
        return rc(gs.at[lax.rem(ym + d, NY)], gr.at[dst], gw_s.at[d - 1], gw_r.at[d - 1], tp=ydev(d))

    def weight_gradients():
        for m in range(3):
            grad = 0.0
            for c in range(NC):
                lhs = act[c][:, :, m * u : (m + 1) * u].reshape(CHUNKS[c] * cp, u)
                grad = grad + dot(lhs, rows[c][1 if m == 2 else 0], 0, 0)
            gs[:, m] = grad.reshape(NY, 64, yb).astype(BF)
        for d in (1, 3, 2):
            go(gwcopy(d, ym))
        gr[ym] = gs[ym]

    stages = (stage_a, stage_b, stage_c, stage_d, stage_e, stage_f, stage_g, stage_h, stage_i)
    for step in range(LAG * (NC - 1) + len(stages)):
        for c in range(NC):
            k = step - LAG * c
            if 0 <= k < len(stages):
                stages[k](c)
                if c == NC - 1 and k == 6:
                    weight_gradients()

    wait_halo = rc(mhs, mh, h_s.at[0], h_r.at[0], sp=lax.rem(me + 1, ns))
    wait_halo.wait_recv()
    prev = jnp.where(me == 0, 0.0, mh[...])
    ext = jnp.concatenate([prev, mixed], axis=0)
    tap = taps_ref[...]
    conv = tap[2:3] * mixed + tap[1:2] * ext[7 : 7 + t] + tap[0:1] * ext[6 : 6 + t]
    merged = (gb_ref[...].astype(F32) * conv).astype(BF)

    @pl.loop(1, ns)
    def _(d):
        i = lax.rem(me + d, ns)
        rc(ret.at[i], retr.at[i], r_s.at[i], r_r.at[i], sp=i).wait_recv()

    back_rows = retr[...].astype(F32).reshape(n_rows, W).astype(BF)
    grad_cols = ccol[...].astype(F32) + dot(pt[...], back_rows, 1, 0)
    st[tp] = grad_cols.astype(BF)

    def stcopy(dx, dy):
        to = lax.rem(ym + dy, NY) * NX + lax.rem(xm + NX - dx, NX)
        return rc(st.at[tp], st.at[tp], st_s.at[dx, dy], st_r.at[tp], tp=to)

    for dx in ORDER:
        for dy in (1, 3, 2, 0):
            if dx or dy:
                go(stcopy(dx, dy))

    for d in (1, 2, 3):
        gwcopy(d, lax.rem(ym - d + NY, NY)).wait_recv()
    for m, out in enumerate((gg_out, gu_out, gd_out)):
        for yy in range(NY):
            out[:, yy * yb : (yy + 1) * yb] = gr[yy, m].astype(F32)
    load_o.wait()

    def pair(g):
        return rc(gpp.at[g], pr.at[g], p_s.at[g], p_r.at[g], sp=zm * 2 + 1 - core)

    def onward(z):
        return rc(gq.at[z], fr.at[zm], f_s.at[z], f_r.at[zm], sp=z * 2 + core)

    def send_sums(g):
        pair(g).wait_recv()
        for yy in range(NY):
            z = yy * NX + lax.rem(xm + ORDER[g], NX)
            gq[z] = (gpo[g, yy] + pr[g, yy].astype(F32)).astype(BF)

            @pl.when(z != zm)
            def _(z=z):
                onward(z).start()

    for g, dx in enumerate(ORDER):
        xx = lax.rem(xm + dx, NX)
        for dy in range(NY):
            if dx or dy:
                src = lax.rem(ym + dy, NY) * NX + xx
                rc(st.at[tp], st.at[src], st_s.at[dx, dy], st_r.at[src], tp=src).wait_recv()
        block = jnp.concatenate([st[yy * NX + xx] for yy in range(NY)], axis=1)
        proj = dot(block, merged, 0, 0).reshape(NY, 2, 64, W)
        proj0 = proj[:, 0]
        proj1 = proj[:, 1]
        gpo[g] = jnp.where(core == 0, proj0, proj1)
        gpp[g] = jnp.where(core == 0, proj1, proj0).astype(BF)
        pair(g).start()
        if g:
            send_sums(g - 1)

    stream = jnp.concatenate([st[j] for j in range(NX * NY)], axis=1)
    grad_merged = dot(stream, opv[...], 1, 1)
    grad_conv = grad_merged * gb_ref[...].astype(F32)
    ghs[...] = grad_conv[0:8, :]
    halo_g = rc(ghs, gh, h_s.at[1], h_r.at[1], sp=lax.rem(me + ns - 1, ns))
    halo_g.start()
    send_sums(NX - 1)
    ggb_out[...] = (grad_merged * conv).astype(BF)

    halo_g.wait_recv()
    following = jnp.where(me == ns - 1, 0.0, gh[...])
    extg = jnp.concatenate([grad_conv, following], axis=0)
    grad_mixed = tap[2:3] * grad_conv + tap[1:2] * extg[1 : 1 + t] + tap[0:1] * extg[2 : 2 + t]
    ggc_out[...] = (grad_mixed * ci_ref[...].astype(F32)).astype(BF)
    gci_out[...] = (grad_mixed * gc_ref[...].astype(F32)).astype(BF)

    dispatch(1 - core).wait_send()
    giveback(1 - core).wait_send()

    @pl.loop(2, ns)
    def _(j):
        dispatch(j).wait_send()
        giveback(j).wait_send()

    halo_g.wait_send()
    for g in range(NX):
        pair(g).wait_send()
    for copy in sends:
        copy.wait_send()

    @pl.loop(1, nz)
    def _(d):
        z = lax.rem(zm + d, nz)
        rc(gq.at[z], fr.at[z], f_s.at[z], f_r.at[z], sp=z * 2 + core).wait()

    fr[zm] = gq[zm]
    gp_out[...] = jnp.sum(fr[...].astype(F32), axis=0)


def write_out(n, *refs):
    sems = refs[-1]
    copies = [pltpu.make_async_copy(refs[k], refs[n + k], sems.at[k]) for k in range(n)]
    for copy in copies:
        copy.start()
    for copy in copies:
        copy.wait()


def on_device(
    moe_input, cotangent, route_ids, route_weights, expert_gate, expert_up, expert_down,
    out_proj, gate_b, gate_c, conv_in, taps,
):
    ns = lax.axis_size("sp")
    t, model = moe_input.shape
    cap = 2 * t * route_ids.shape[1] // ns
    cp = -(-cap // 8) * 8
    n_rows = ns * cp
    yb = model // NY
    tpn = NX * NY
    units = expert_gate.shape[2]
    sds = jax.ShapeDtypeStruct
    vmem = pl.BlockSpec(memory_space=pltpu.VMEM)
    anym = pl.BlockSpec(memory_space=pltpu.HBM)
    dma = pltpu.SemaphoreType.DMA
    V = pltpu.VMEM

    def each(buffer):
        return tuple(buffer(pc * cp) for pc in CHUNKS)

    scratch = [
        V((2, t), jnp.int32), V((2, t), F32), V((t, W), BF), V((t, W), BF), V((t, W), BF), V((3, W), F32),
        V((t, W), BF), V((t, W), BF), V((W, model), BF), V((ns, 2, cp, W), BF), V((NX, ns, 2, cp, W), BF),
        V((NY, 3, units, yb), BF),
        each(lambda r: V((2, r, yb), BF)), each(lambda r: V((NY, r // 4, 6 * W), BF)), each(lambda r: V((r // 4, 6 * W), BF)),
        each(lambda r: V((2, r // 4, 6 * W), BF)), each(lambda r: V((NY, r // 4, 6 * W), BF)), each(lambda r: V((NX, r, W), BF)),
        each(lambda r: V((2, r // 2, W), BF)), each(lambda r: V((2, r, W), BF)),
        V((ns, cp, W), BF), V((ns, cp, W), BF), V((t, n_rows), BF), V((tpn, t, W), BF),
        V((NY, 3, units, yb), BF), V((NY, 3, units, yb), BF), V((8, W), F32), V((8, W), F32), V((8, W), F32), V((8, W), F32),
        V((NX, NY, 64, W), F32), V((NX, NY, 64, W), BF), V((NX, NY, 64, W), BF), V((tpn, 64, W), BF), V((tpn, 64, W), BF),
        dma((9,)), dma((3,)), dma((3, 3)), dma((3, 3)), dma((ns,)), dma((ns,)), dma((NC, 2)), dma((NC, 2)), dma((NC, 2)), dma((NC, 2)),
        dma((NC, 6)), dma((NC, 6)), dma((NC, 2)), dma((NC, 2)), dma((NC, 2)), dma((NC, 2)),
        dma((NC, 6)), dma((NC, 6)), dma((ns,)), dma((ns,)), dma((NX, NY)), dma((tpn,)), dma((3,)), dma((3,)), dma((2,)), dma((2,)),
        dma((NX,)), dma((NX,)), dma((ns // 2,)), dma((ns // 2,)),
    ]
    out_shape = (
        sds((units, model), F32), sds((units, model), F32), sds((units, model), F32), sds((64, W), F32),
        sds((t, W), BF), sds((t, W), BF), sds((t, W), BF),
    )
    outs = pl.pallas_call(
        functools.partial(kernel, ns, cp),
        out_shape=tuple(pltpu.VMEM(o.shape, o.dtype) for o in out_shape),
        in_specs=[anym] * 12,
        out_specs=[vmem] * 7,
        scratch_shapes=scratch,
        compiler_params=pltpu.CompilerParams(collective_id=0, has_side_effects=True, vmem_limit_bytes=40 * 2**20),
    )(
        *(
            pltpu.with_memory_space_constraint(a, pltpu.HBM)
            for a in (
                route_ids.T, route_weights.T, moe_input, cotangent, expert_gate[0].T, expert_up[0].T, expert_down[0],
                out_proj, gate_b, gate_c, conv_in, taps,
            )
        )
    )
    outs = pl.pallas_call(
        functools.partial(write_out, 7),
        out_shape=tuple(pltpu.HBM(o.shape, o.dtype) for o in out_shape),
        in_specs=[vmem] * 7,
        out_specs=[anym] * 7,
        scratch_shapes=[dma((7,))],
    )(*(pltpu.with_memory_space_constraint(o, pltpu.VMEM) for o in outs))
    gg, gu, gd, gp, ggb, ggc, gci = outs
    return gg.T[None], gu.T[None], gd[None], gp.T, ggb, ggc, gci


def solution(mesh):
    row, cols = P("sp", None), P("sp", "tp")
    return jax.shard_map(
        on_device,
        mesh=mesh,
        in_specs=(
            row, row, row, row, P("sp", None, "tp"), P("sp", None, "tp"), P("sp", "tp", None), P("tp", None),
            cols, cols, cols, P(None, "tp"),
        ),
        out_specs=(
            P("sp", None, "tp"), P("sp", None, "tp"), P("sp", "tp", None), P("tp", "sp"), cols, cols, cols,
        ),
        check_vma=False,
    )
```

```python
import functools

import jax
import jax.numpy as jnp
from jax import lax
from jax.experimental import pallas as pl
from jax.experimental.pallas import tpu as pltpu
from jax.sharding import PartitionSpec as P

MESH = pl.DeviceIdType.MESH
BF = jnp.bfloat16
F32 = jnp.float32
NX = 4
NY = 4
W = 128


def dot(a, b, ca, cb):
    return lax.dot_general(a, b, (((ca,), (cb,)), ((), ())), preferred_element_type=F32)


CHUNKS = (8, 8, 8, 8)
RANGES = (0, 3, 2, 1)
NEAR = RANGES.index(0)
STARTS = tuple(sum(CHUNKS[:k]) for k in range(len(CHUNKS)))
NC = len(CHUNKS)
SEQUENCE = "a0 c0 a1 e0 a2 c1 a3 g0 c2 e1 c3 g1 e2 i0 e3 g2 i1 g3 i2 i3"
ORDER = (0, 1, 3, 2)
SENDS = (2, 1, 3)


def kernel(
    ns, cp,
    ids_hbm, wts_hbm, x_hbm, c_hbm, wg_hbm, wu_hbm, wd_hbm, op_hbm, gb_hbm, gc_hbm, ci_hbm, taps_hbm,
    gg_out, gu_out, gd_out, gp_out, ggb_out, ggc_out, gci_out,
    ids_ref, wts_ref, gb_ref, gc_ref, ci_ref, taps_ref,
    xcol, ccol, opv, disp, gx, wx, rows, preb, rs, act, hid, slotp, xr, ret, retr, pt, st,
    gs, gr, mhs, mh, ghs, gh, gpo, gpp, pr, gq, fr,
    loc_sem, bsem_w, wsem_s, wsem_r, d_s, d_r, gx_s, gx_r, y_s, y_r, a_s, a_r, hd_s, hd_r,
    xs_s, xs_r, r_s, r_r, st_s, st_r, fw_s, fw_r, gw_s, gw_r, h_s, h_r, p_s, p_r, f_s, f_r,
):
    me = lax.axis_index("sp")
    tp = lax.axis_index("tp")
    ym = lax.div(tp, NX)
    xm = lax.rem(tp, NX)
    core = lax.rem(me, 2)
    zm = lax.div(me, 2)
    nz = ns // 2
    t = ids_ref.shape[1]
    n_rows = ns * cp
    u = 2 * W
    yb = 4 * W

    def xdev(d):
        return ym * NX + lax.rem(xm + d, NX)

    def ydev(d):
        return lax.rem(ym + d, NY) * NX + xm

    def rc(src, dst, ss, rs, **where):
        return pltpu.make_async_remote_copy(
            src_ref=src, dst_ref=dst, send_sem=ss, recv_sem=rs, device_id=where, device_id_type=MESH
        )

    def offset(k):
        return lax.div(k + 1, 2) * (2 * lax.rem(k, 2) - 1)

    sends = []

    def go(copy):
        copy.start()
        sends.append(copy)

    barrier = pltpu.get_barrier_semaphore()
    small = [
        pltpu.make_async_copy(src, dst, loc_sem.at[k])
        for k, (src, dst) in enumerate(
            (
                (ids_hbm, ids_ref), (wts_hbm, wts_ref), (gb_hbm, gb_ref), (gc_hbm, gc_ref), (ci_hbm, ci_ref),
                (taps_hbm, taps_ref),
            )
        )
    ]
    cols = pl.ds(pl.multiple_of(tp * W, W), W)
    load_x = pltpu.make_async_copy(x_hbm.at[:, cols], xcol, loc_sem.at[6])
    load_c = pltpu.make_async_copy(c_hbm.at[:, cols], ccol, loc_sem.at[7])
    load_o = pltpu.make_async_copy(op_hbm, opv, loc_sem.at[8])
    mats = (wg_hbm, wu_hbm, wd_hbm)
    ycols = pl.ds(pl.multiple_of(ym * yb, yb), yb)
    load_w = [pltpu.make_async_copy(mats[m].at[:, ycols], wx.at[ym, m], bsem_w.at[m]) for m in range(3)]
    small[0].start()
    small[1].start()
    load_x.start()
    load_c.start()

    @pl.loop(1, ns)
    def _(d):
        pl.semaphore_signal(barrier, inc=1, device_id={"sp": lax.rem(me + d, ns)}, device_id_type=MESH)

    @pl.loop(1, NX * NY)
    def _(d):
        pl.semaphore_signal(barrier, inc=1, device_id={"tp": lax.rem(tp + d, NX * NY)}, device_id_type=MESH)

    for copy in small[2:]:
        copy.start()
    for copy in load_w:
        copy.start()
    load_o.start()

    small[0].wait()
    small[1].wait()
    id0 = ids_ref[0:1, :]
    id1 = ids_ref[1:2, :]
    eio = lax.broadcasted_iota(jnp.int32, (ns, t), 0)
    oh0 = (eio == id0).astype(F32)
    oh1 = (eio == id1).astype(F32)
    before = (lax.broadcasted_iota(jnp.int32, (t, t), 0) < lax.broadcasted_iota(jnp.int32, (t, t), 1)).astype(F32).astype(BF)
    cum = dot((oh0 + oh1).astype(BF), before, 1, 0)
    slot0 = id0 * cp + jnp.sum(oh0 * cum, axis=0, keepdims=True).astype(jnp.int32)
    slot1 = id1 * cp + jnp.sum(oh1 * cum, axis=0, keepdims=True).astype(jnp.int32)
    rio = lax.broadcasted_iota(jnp.int32, (n_rows, t), 0)
    p0 = rio == slot0
    p1 = rio == slot1
    pmat = jnp.where(p0 | p1, 1.0, 0.0)
    wslot = jnp.sum(jnp.where(p0, wts_ref[0:1, :], jnp.where(p1, wts_ref[1:2, :], 0.0)), axis=1, keepdims=True)
    pb = pmat.astype(BF)
    load_x.wait()
    load_c.wait()
    picked = dot(pb, jnp.concatenate([xcol[...], ccol[...]], axis=1), 1, 0)
    disp[:, 0] = picked[:, :W].reshape(ns, cp, W).astype(BF)
    disp[:, 1] = (wslot * picked[:, W:]).reshape(ns, cp, W).astype(BF)

    for copy in small[2:]:
        copy.wait()
    mixed = gc_ref[...].astype(F32) * ci_ref[...].astype(F32)
    mhs[...] = mixed[t - 8 :, :]

    pl.semaphore_wait(barrier, ns - 1 + NX * NY - 1)

    def distance(c, j):
        return offset(RANGES[c] * 4 + lax.div(j, 2))

    def dispatch(c, j):
        i = lax.rem(zm - distance(c, j) + nz, nz) * 2 + lax.rem(j, 2)
        place = STARTS[c] + j - lax.rem(j, 2) + core
        return rc(disp.at[i], gx.at[xm, place], d_s.at[STARTS[c] + j], d_r.at[place], sp=i)

    def arrival(p):
        return rc(disp.at[p], gx.at[xm, p], d_s.at[p], d_r.at[p], sp=lax.rem(me + 1, ns))

    def each_place(c, act_on):
        if c == NEAR:
            act_on(1 - core)

        @pl.loop(2 if c == NEAR else 0, CHUNKS[c])
        def _(j):
            act_on(j)

    own_place = STARTS[NEAR] + core
    for c in range(NC):
        each_place(c, lambda j, c=c: dispatch(c, j).start())

    def wcopy(d, m, dst):
        block = pl.ds(pl.multiple_of(lax.rem(ym + d, NY) * yb, yb), yb)
        return rc(mats[m].at[:, block], wx.at[dst, m], wsem_s.at[d - 1, m], wsem_r.at[d - 1, m], tp=ydev(d))

    for d in (1, 3, 2):
        for m in range(3):
            go(wcopy(d, m, ym))

    halo_m = rc(mhs, mh, h_s.at[0], h_r.at[0], sp=lax.rem(me + 1, ns))
    go(halo_m)

    gx[xm, own_place] = disp[me]

    pt[...] = pmat.T.astype(BF)

    def wait_on(dst, ss, rs):
        rc(dst, dst, ss, rs, tp=xdev(1)).wait_recv()

    weights = []

    def stage_a(c):
        at, pc = STARTS[c], CHUNKS[c]
        each_place(c, lambda j: arrival(at + j).wait_recv())
        part = gx.at[xm, pl.ds(at, pc)]
        for d in SENDS:
            go(rc(part, part, gx_s.at[c, d - 1], gx_r.at[c, d - 1], tp=xdev(d)))

    def stage_c(c):
        at, pc = STARTS[c], CHUNKS[c]
        qr = pc * cp
        yq = qr // NY
        if c == 0:
            for m in range(3):
                load_w[m].wait()
                for d in (1, 2, 3):
                    wcopy(d, m, lax.rem(ym - d + NY, NY)).wait_recv()
            weights.extend(jnp.concatenate([wx[yy, m] for yy in range(NY)], axis=0) for m in range(3))
        for d in SENDS:
            wait_on(gx.at[lax.rem(xm + NX - d, NX), pl.ds(at, pc)], gx_s.at[c, d - 1], gx_r.at[c, d - 1])
        for s in range(2):
            blocks = [gx[xx, at : at + pc, s].astype(F32).reshape(qr, W) for xx in range(NX)]
            rows[c][s] = jnp.concatenate(blocks, axis=1).astype(BF)
        for m in range(3):
            pre = dot(rows[c][1 if m == 2 else 0], weights[m], 1, 1)
            preb[c][:, :, m * u : (m + 1) * u] = pre.reshape(NY, yq, u).astype(BF)
        for d in SENDS:
            to = lax.rem(ym + d, NY)
            go(rc(preb[c].at[to], rs[c].at[d - 1], y_s.at[c, d - 1], y_r.at[c, d - 1], tp=ydev(d)))

    def stage_e(c):
        for d in SENDS:
            wait_on(rs[c].at[d - 1], y_s.at[c, d - 1], y_r.at[c, d - 1])

        def total(m):
            q = slice(m * u, (m + 1) * u)
            return preb[c][ym, :, q].astype(F32) + sum(rs[c][k, :, q].astype(F32) for k in range(3))

        pre_gate = total(0)
        pre_up = total(1)
        back = total(2)
        sigma = jax.nn.sigmoid(pre_gate)
        active = pre_gate * sigma
        act[c][ym, :, 0:u] = (back * pre_up * sigma * (1.0 + pre_gate * (1.0 - sigma))).astype(BF)
        act[c][ym, :, u : 2 * u] = (back * active).astype(BF)
        hid[c][ym] = (active * pre_up).astype(BF)
        own = act[c].at[ym]
        for d in SENDS:
            go(rc(own, own, a_s.at[c, d - 1], a_r.at[c, d - 1], tp=ydev(d)))

    def stage_g(c):
        qr = CHUNKS[c] * cp
        for d in SENDS:
            wait_on(act[c].at[lax.rem(ym + NY - d, NY)], a_s.at[c, d - 1], a_r.at[c, d - 1])
        part = dot(act[c][:, :, 0:u].reshape(qr, u), weights[0], 1, 0)
        part = part + dot(act[c][:, :, u : 2 * u].reshape(qr, u), weights[1], 1, 0)
        for xx in range(NX):
            slotp[c][xx] = part[:, xx * W : (xx + 1) * W].astype(BF)
        for d in SENDS:
            to = lax.rem(xm + d, NX)
            go(rc(slotp[c].at[to], xr[c].at[d - 1], xs_s.at[c, d - 1], xs_r.at[c, d - 1], tp=xdev(d)))

    def giveback(c, j):
        p = STARTS[c] + j
        i = lax.rem(zm + distance(c, j) + nz, nz) * 2 + lax.rem(j, 2)
        return rc(ret.at[p], retr.at[me], r_s.at[p], r_r.at[me], sp=i)

    def stage_i(c):
        at, pc = STARTS[c], CHUNKS[c]
        for d in SENDS:
            wait_on(xr[c].at[d - 1], xs_s.at[c, d - 1], xs_r.at[c, d - 1])
        slot = slotp[c][xm].astype(F32) + sum(xr[c][k].astype(F32) for k in range(3))
        ret[at : at + pc] = slot.reshape(pc, cp, W).astype(BF)
        if c == NEAR:
            retr[me] = ret[own_place]
        each_place(c, lambda j: giveback(c, j).start())

    def gwcopy(d, dst, k):
        part = pl.ds(2 * k, 2 - k)
        return rc(gs.at[lax.rem(ym + d, NY), part], gr.at[dst, part], gw_s.at[d - 1, k], gw_r.at[d - 1, k], tp=ydev(d))

    def weight_gradient(m, lefts):
        grad = 0.0
        for c in range(NC):
            left = lefts[c][:, :, m * u : (m + 1) * u] if m < 2 else lefts[c][...]
            grad = grad + dot(left.reshape(CHUNKS[c] * cp, u), rows[c][1 if m == 2 else 0], 0, 0)
        gs[:, m] = grad.reshape(NY, 64, yb).astype(BF)

    def gate_and_up():
        for c in range(NC):
            own = hid[c].at[ym]
            for d in SENDS:
                go(rc(own, own, hd_s.at[c, d - 1], hd_r.at[c, d - 1], tp=ydev(d)))
        for m in range(2):
            weight_gradient(m, act)
        for d in SENDS:
            go(gwcopy(d, ym, 0))

    def down():
        for c in range(NC):
            for d in SENDS:
                wait_on(hid[c].at[lax.rem(ym + NY - d, NY)], hd_s.at[c, d - 1], hd_r.at[c, d - 1])
        weight_gradient(2, hid)
        for d in SENDS:
            go(gwcopy(d, ym, 1))
        gr[ym] = gs[ym]

    stages = (stage_a, stage_c, stage_e, stage_g, stage_i)
    for item in SEQUENCE.split():
        k, c = "acegi".index(item[0]), int(item[1])
        stages[k](c)
        if k == 3 and c == NC - 1:
            gate_and_up()
    wait_halo = rc(mhs, mh, h_s.at[0], h_r.at[0], sp=lax.rem(me + 1, ns))
    wait_halo.wait_recv()
    prev = jnp.where(me == 0, 0.0, mh[...])
    ext = jnp.concatenate([prev, mixed], axis=0)
    tap = taps_ref[...]
    conv = tap[2:3] * mixed + tap[1:2] * ext[7 : 7 + t] + tap[0:1] * ext[6 : 6 + t]
    merged = (gb_ref[...].astype(F32) * conv).astype(BF)

    @pl.loop(1, ns)
    def _(d):
        i = lax.rem(me + d, ns)
        rc(ret.at[i], retr.at[i], r_s.at[i], r_r.at[i], sp=i).wait_recv()

    back_rows = retr[...].astype(F32).reshape(n_rows, W).astype(BF)
    grad_cols = ccol[...].astype(F32) + dot(pt[...], back_rows, 1, 0)
    st[tp] = grad_cols.astype(BF)

    cut = -(-t // 32) * 16
    first, rest = pl.ds(0, cut), pl.ds(cut, t - cut)

    for d in SENDS:
        go(rc(st.at[tp], st.at[tp], st_s.at[0, d], st_r.at[tp], tp=ydev(d)))
        go(rc(st.at[tp], st.at[tp], st_s.at[1, d], st_r.at[tp], tp=xdev(d)))
    for d in SENDS:
        src = ydev(NY - d)
        wait_on(st.at[src], st_s.at[0, d], st_r.at[src])
        for e in SENDS:
            go(rc(st.at[src, first], st.at[src, first], fw_s.at[0, d, e], fw_r.at[0, src], tp=xdev(e)))
    for d in SENDS:
        src = xdev(NX - d)
        wait_on(st.at[src], st_s.at[1, d], st_r.at[src])
        for e in SENDS:
            go(rc(st.at[src, rest], st.at[src, rest], fw_s.at[1, d, e], fw_r.at[1, src], tp=ydev(e)))

    load_o.wait()

    def pair(g):
        return rc(gpp.at[g], pr.at[g], p_s.at[g], p_r.at[g], sp=zm * 2 + 1 - core)

    def onward(z):
        return rc(gq.at[z], fr.at[zm], f_s.at[z], f_r.at[zm], sp=z * 2 + core)

    def send_sums(g):
        pair(g).wait_recv()
        for far in (2, 1, 3, 0):
            yy = lax.rem(lax.div(zm, NX) + far, NY)
            z = yy * NX + lax.rem(xm + ORDER[g], NX)
            gq[z] = (gpo[g, yy] + pr[g, yy].astype(F32)).astype(BF)

            @pl.when(z != zm)
            def _(z=z):
                onward(z).start()

    for g, dx in enumerate(ORDER):
        xx = lax.rem(xm + dx, NX)
        for dy in range(NY):
            if dx and dy:
                src = lax.rem(ym + dy, NY) * NX + xx
                wait_on(st.at[src, first], fw_s.at[0, 1, 1], fw_r.at[0, src])
                wait_on(st.at[src, rest], fw_s.at[1, 1, 1], fw_r.at[1, src])
        block = jnp.concatenate([st[yy * NX + xx] for yy in range(NY)], axis=1)
        proj = dot(block, merged, 0, 0).reshape(NY, 2, 64, W)
        proj0 = proj[:, 0]
        proj1 = proj[:, 1]
        gpo[g] = jnp.where(core == 0, proj0, proj1)
        gpp[g] = jnp.where(core == 0, proj1, proj0).astype(BF)
        pair(g).start()
        if g == 0:
            send_sums(0)
        elif g > 1:
            send_sums(g - 1)

    stream = jnp.concatenate([st[j] for j in range(NX * NY)], axis=1)
    grad_merged = dot(stream, opv[...], 1, 1)
    grad_conv = grad_merged * gb_ref[...].astype(F32)
    ghs[...] = grad_conv[0:8, :]
    halo_g = rc(ghs, gh, h_s.at[1], h_r.at[1], sp=lax.rem(me + ns - 1, ns))
    halo_g.start()
    send_sums(NX - 1)
    ggb_out[...] = (grad_merged * conv).astype(BF)
    down()

    halo_g.wait_recv()
    following = jnp.where(me == ns - 1, 0.0, gh[...])
    extg = jnp.concatenate([grad_conv, following], axis=0)
    grad_mixed = tap[2:3] * grad_conv + tap[1:2] * extg[1 : 1 + t] + tap[0:1] * extg[2 : 2 + t]
    ggc_out[...] = (grad_mixed * ci_ref[...].astype(F32)).astype(BF)
    gci_out[...] = (grad_mixed * gc_ref[...].astype(F32)).astype(BF)

    for k in range(2):
        for d in SENDS:
            gwcopy(d, lax.rem(ym - d + NY, NY), k).wait_recv()
    for m, out in enumerate((gg_out, gu_out, gd_out)):
        for yy in range(NY):
            out[:, yy * yb : (yy + 1) * yb] = gr[yy, m].astype(F32)
    for c in range(NC):
        each_place(c, lambda j, c=c: dispatch(c, j).wait_send())
        each_place(c, lambda j, c=c: giveback(c, j).wait_send())

    halo_g.wait_send()
    for g in range(NX):
        pair(g).wait_send()
    for copy in sends:
        copy.wait_send()

    @pl.loop(1, nz)
    def _(d):
        z = lax.rem(zm + d, nz)
        rc(gq.at[z], fr.at[z], f_s.at[z], f_r.at[z], sp=z * 2 + core).wait()

    fr[zm] = gq[zm]
    gp_out[...] = jnp.sum(fr[...].astype(F32), axis=0)


def write_out(n, *refs):
    sems = refs[-1]
    copies = [pltpu.make_async_copy(refs[k], refs[n + k], sems.at[k]) for k in range(n)]
    for copy in copies:
        copy.start()
    for copy in copies:
        copy.wait()


def on_device(
    moe_input, cotangent, route_ids, route_weights, expert_gate, expert_up, expert_down,
    out_proj, gate_b, gate_c, conv_in, taps,
):
    ns = lax.axis_size("sp")
    t, model = moe_input.shape
    cap = 2 * t * route_ids.shape[1] // ns
    cp = -(-cap // 8) * 8
    n_rows = ns * cp
    yb = model // NY
    tpn = NX * NY
    units = expert_gate.shape[2]
    sds = jax.ShapeDtypeStruct
    vmem = pl.BlockSpec(memory_space=pltpu.VMEM)
    anym = pl.BlockSpec(memory_space=pltpu.HBM)
    dma = pltpu.SemaphoreType.DMA
    V = pltpu.VMEM

    def each(buffer):
        return tuple(buffer(pc * cp) for pc in CHUNKS)

    scratch = [
        V((2, t), jnp.int32), V((2, t), F32), V((t, W), BF), V((t, W), BF), V((t, W), BF), V((3, W), F32),
        V((t, W), BF), V((t, W), BF), V((W, model), BF), V((ns, 2, cp, W), BF), V((NX, ns, 2, cp, W), BF),
        V((NY, 3, units, yb), BF),
        each(lambda r: V((2, r, yb), BF)), each(lambda r: V((NY, r // 4, 6 * W), BF)), each(lambda r: V((3, r // 4, 6 * W), BF)),
        each(lambda r: V((NY, r // 4, 4 * W), BF)), each(lambda r: V((NY, r // 4, 2 * W), BF)), each(lambda r: V((NX, r, W), BF)),
        each(lambda r: V((3, r, W), BF)),
        V((ns, cp, W), BF), V((ns, cp, W), BF), V((t, n_rows), BF), V((tpn, t, W), BF),
        V((NY, 3, units, yb), BF), V((NY, 3, units, yb), BF), V((8, W), F32), V((8, W), F32), V((8, W), F32), V((8, W), F32),
        V((NX, NY, 64, W), F32), V((NX, NY, 64, W), BF), V((NX, NY, 64, W), BF), V((tpn, 64, W), BF), V((tpn, 64, W), BF),
        dma((9,)), dma((3,)), dma((3, 3)), dma((3, 3)), dma((ns,)), dma((ns,)), dma((NC, 3)), dma((NC, 3)),
        dma((NC, 3)), dma((NC, 3)), dma((NC, 3)), dma((NC, 3)), dma((NC, 3)), dma((NC, 3)), dma((NC, 3)), dma((NC, 3)),
        dma((ns,)), dma((ns,)), dma((2, NX)), dma((tpn,)), dma((2, NY, NX)), dma((2, tpn)), dma((3, 2)), dma((3, 2)), dma((2,)), dma((2,)),
        dma((NX,)), dma((NX,)), dma((ns // 2,)), dma((ns // 2,)),
    ]
    out_shape = (
        sds((units, model), F32), sds((units, model), F32), sds((units, model), F32), sds((64, W), F32),
        sds((t, W), BF), sds((t, W), BF), sds((t, W), BF),
    )
    outs = pl.pallas_call(
        functools.partial(kernel, ns, cp),
        out_shape=tuple(pltpu.VMEM(o.shape, o.dtype) for o in out_shape),
        in_specs=[anym] * 12,
        out_specs=[vmem] * 7,
        scratch_shapes=scratch,
        compiler_params=pltpu.CompilerParams(collective_id=0, has_side_effects=True, vmem_limit_bytes=40 * 2**20),
    )(
        *(
            pltpu.with_memory_space_constraint(a, pltpu.HBM)
            for a in (
                route_ids.T, route_weights.T, moe_input, cotangent, expert_gate[0].T, expert_up[0].T, expert_down[0],
                out_proj, gate_b, gate_c, conv_in, taps,
            )
        )
    )
    outs = pl.pallas_call(
        functools.partial(write_out, 7),
        out_shape=tuple(pltpu.HBM(o.shape, o.dtype) for o in out_shape),
        in_specs=[vmem] * 7,
        out_specs=[anym] * 7,
        scratch_shapes=[dma((7,))],
    )(*(pltpu.with_memory_space_constraint(o, pltpu.VMEM) for o in outs))
    gg, gu, gd, gp, ggb, ggc, gci = outs
    return gg.T[None], gu.T[None], gd[None], gp.T, ggb, ggc, gci


def solution(mesh):
    row, cols = P("sp", None), P("sp", "tp")
    return jax.shard_map(
        on_device,
        mesh=mesh,
        in_specs=(
            row, row, row, row, P("sp", None, "tp"), P("sp", None, "tp"), P("sp", "tp", None), P("tp", None),
            cols, cols, cols, P(None, "tp"),
        ),
        out_specs=(
            P("sp", None, "tp"), P("sp", None, "tp"), P("sp", "tp", None), P("tp", "sp"), cols, cols, cols,
        ),
        check_vma=False,
    )
```

```python
import functools

import jax
import jax.numpy as jnp
from jax import lax
from jax.experimental import pallas as pl
from jax.experimental.pallas import tpu as pltpu
from jax.sharding import PartitionSpec as P

MESH = pl.DeviceIdType.MESH
BF = jnp.bfloat16
F32 = jnp.float32
NX = 4
NY = 4
W = 128


def dot(a, b, ca, cb):
    return lax.dot_general(a, b, (((ca,), (cb,)), ((), ())), preferred_element_type=F32)


CHUNKS = (8, 8, 8, 8)
RANGES = (0, 3, 2, 1)
NEAR = RANGES.index(0)
STARTS = tuple(sum(CHUNKS[:k]) for k in range(len(CHUNKS)))
NC = len(CHUNKS)
SEQUENCE = (
    (0, 0), (1, 0), (0, 1), (2, 0), (0, 2), (1, 1), (0, 3), (3, 0), (1, 2), (2, 1),
    (1, 3), (3, 1), (2, 2), (4, 0), (2, 3), (3, 2), (4, 1), (3, 3), (4, 2), (4, 3),
)
ORDER = (0, 1, 3, 2)
SENDS = (2, 1, 3)


def kernel(
    ns, cp,
    ids_hbm, wts_hbm, x_hbm, c_hbm, wg_hbm, wu_hbm, wd_hbm, op_hbm, gb_hbm, gc_hbm, ci_hbm, taps_hbm,
    gg_any, gu_any, gd_any, gp_any, ggb_any, ggc_any, gci_any,
    gg_out, gu_out, gd_out, gp_out, ggb_out, ggc_out, gci_out, out_sem,
    ids_ref, wts_ref, gb_ref, gc_ref, ci_ref, taps_ref,
    xcol, ccol, opv, disp, gx, wx, rows, preb, rs, act, hid, slotp, xr, ret, retr, pt, st,
    gs, gr, mhs, mh, ghs, gh, gpo, gpp, pr, gq, fr,
    loc_sem, bsem_w, wsem_s, wsem_r, d_s, d_r, gx_s, gx_r, y_s, y_r, a_s, a_r, hd_s, hd_r,
    xs_s, xs_r, r_s, r_r, st_s, st_r, fw_s, fw_r, gw_s, gw_r, h_s, h_r, p_s, p_r, f_s, f_r,
):
    me = lax.axis_index("sp")
    tp = lax.axis_index("tp")
    ym = lax.div(tp, NX)
    xm = lax.rem(tp, NX)
    core = lax.rem(me, 2)
    zm = lax.div(me, 2)
    nz = ns // 2
    t = ids_ref.shape[1]
    n_rows = ns * cp
    u = 2 * W
    yb = 4 * W

    def xdev(d):
        return ym * NX + lax.rem(xm + d, NX)

    def ydev(d):
        return lax.rem(ym + d, NY) * NX + xm

    def rc(src, dst, ss, rs, **where):
        return pltpu.make_async_remote_copy(
            src_ref=src, dst_ref=dst, send_sem=ss, recv_sem=rs, device_id=where, device_id_type=MESH
        )

    def offset(k):
        return lax.div(k + 1, 2) * (2 * lax.rem(k, 2) - 1)

    placed = [
        pltpu.make_async_copy(src, dst, out_sem.at[k])
        for k, (src, dst) in enumerate(
            (
                (gg_out, gg_any), (gu_out, gu_any), (gd_out, gd_any), (gp_out, gp_any), (ggb_out, ggb_any),
                (ggc_out, ggc_any), (gci_out, gci_any),
            )
        )
    ]

    def wait_on(buffer, sem):
        rc(buffer, buffer, sem, sem, tp=lax.rem(tp + 1, NX * NY)).wait_recv()

    sent = []

    def go(copy):
        copy.start()

    barrier = pltpu.get_barrier_semaphore()
    small = [
        pltpu.make_async_copy(src, dst, loc_sem.at[k])
        for k, (src, dst) in enumerate(
            (
                (ids_hbm, ids_ref), (wts_hbm, wts_ref), (gb_hbm, gb_ref), (gc_hbm, gc_ref), (ci_hbm, ci_ref),
                (taps_hbm, taps_ref),
            )
        )
    ]
    cols = pl.ds(pl.multiple_of(tp * W, W), W)
    load_x = pltpu.make_async_copy(x_hbm.at[:, cols], xcol, loc_sem.at[6])
    load_c = pltpu.make_async_copy(c_hbm.at[:, cols], ccol, loc_sem.at[7])
    load_o = pltpu.make_async_copy(op_hbm, opv, loc_sem.at[8])
    mats = (wg_hbm, wu_hbm, wd_hbm)
    ycols = pl.ds(pl.multiple_of(ym * yb, yb), yb)
    load_w = [pltpu.make_async_copy(mats[m].at[:, ycols], wx.at[ym, m], bsem_w.at[m]) for m in range(3)]
    small[0].start()
    small[1].start()
    load_x.start()
    load_c.start()

    @pl.loop(1, ns)
    def _(d):
        pl.semaphore_signal(barrier, inc=1, device_id={"sp": lax.rem(me + d, ns)}, device_id_type=MESH)

    @pl.loop(1, NX * NY)
    def _(d):
        pl.semaphore_signal(barrier, inc=1, device_id={"tp": lax.rem(tp + d, NX * NY)}, device_id_type=MESH)

    for copy in small[2:]:
        copy.start()
    for copy in load_w:
        copy.start()
    load_o.start()

    small[0].wait()
    small[1].wait()
    id0 = ids_ref[0:1, :]
    id1 = ids_ref[1:2, :]
    eio = lax.broadcasted_iota(jnp.int32, (ns, t), 0)
    oh0 = (eio == id0).astype(F32)
    oh1 = (eio == id1).astype(F32)
    before = (lax.broadcasted_iota(jnp.int32, (t, t), 0) < lax.broadcasted_iota(jnp.int32, (t, t), 1)).astype(F32).astype(BF)
    cum = dot((oh0 + oh1).astype(BF), before, 1, 0)
    slot0 = id0 * cp + jnp.sum(oh0 * cum, axis=0, keepdims=True).astype(jnp.int32)
    slot1 = id1 * cp + jnp.sum(oh1 * cum, axis=0, keepdims=True).astype(jnp.int32)
    rio = lax.broadcasted_iota(jnp.int32, (n_rows, t), 0)
    p0 = rio == slot0
    p1 = rio == slot1
    pmat = jnp.where(p0 | p1, 1.0, 0.0)
    wslot = jnp.sum(jnp.where(p0, wts_ref[0:1, :], jnp.where(p1, wts_ref[1:2, :], 0.0)), axis=1, keepdims=True)
    pb = pmat.astype(BF)
    load_x.wait()
    load_c.wait()
    picked = dot(pb, jnp.concatenate([xcol[...], ccol[...]], axis=1), 1, 0)
    disp[:, 0] = picked[:, :W].reshape(ns, cp, W).astype(BF)
    disp[:, 1] = (wslot * picked[:, W:]).reshape(ns, cp, W).astype(BF)

    for copy in small[2:]:
        copy.wait()
    mixed = gc_ref[...].astype(F32) * ci_ref[...].astype(F32)
    mhs[...] = mixed[t - 8 :, :]

    pl.semaphore_wait(barrier, ns - 1 + NX * NY - 1)

    def distance(c, j):
        return offset(RANGES[c] * 4 + lax.div(j, 2))

    def dispatch(c, j):
        i = lax.rem(zm - distance(c, j) + nz, nz) * 2 + lax.rem(j, 2)
        place = STARTS[c] + j - lax.rem(j, 2) + core
        return rc(disp.at[i], gx.at[xm, place], d_s, d_r.at[c], sp=i)

    def each_place(c, act_on):
        if c == NEAR:
            act_on(1 - core)

        @pl.loop(2 if c == NEAR else 0, CHUNKS[c])
        def _(j):
            act_on(j)

    own_place = STARTS[NEAR] + core
    for c in range(NC):
        each_place(c, lambda j, c=c: dispatch(c, j).start())

    def wcopy(d, m, dst):
        block = pl.ds(pl.multiple_of(lax.rem(ym + d, NY) * yb, yb), yb)
        return rc(mats[m].at[:, block], wx.at[dst, m], wsem_s, wsem_r, tp=ydev(d))

    for d in (1, 3, 2):
        for m in range(3):
            go(wcopy(d, m, ym))

    sent.append((wx.at[pl.ds(0, 3)], wsem_s))
    halo_m = rc(mhs, mh, h_s.at[0], h_r.at[0], sp=lax.rem(me + 1, ns))
    halo_m.start()
    sent.append((mhs, h_s.at[0]))
    sent.append((disp.at[pl.ds(0, ns - 1)], d_s))

    gx[xm, own_place] = disp[me]

    pt[...] = pmat.T.astype(BF)

    weights = []

    def stage_a(c):
        at, pc = STARTS[c], CHUNKS[c]
        wait_on(gx.at[xm, pl.ds(at, pc - (c == NEAR))], d_r.at[c])
        part = gx.at[xm, pl.ds(at, pc)]
        for d in SENDS:
            go(rc(part, part, gx_s.at[c], gx_r.at[c], tp=xdev(d)))
        sent.append((gx.at[pl.ds(0, 3), pl.ds(at, pc)], gx_s.at[c]))

    def stage_c(c):
        at, pc = STARTS[c], CHUNKS[c]
        qr = pc * cp
        yq = qr // NY
        if c == 0:
            for m in range(3):
                load_w[m].wait()
            wait_on(wx.at[pl.ds(0, 3)], wsem_r)
            weights.extend(jnp.concatenate([wx[yy, m] for yy in range(NY)], axis=0) for m in range(3))
        wait_on(gx.at[pl.ds(0, 3), pl.ds(at, pc)], gx_r.at[c])
        for s in range(2):
            blocks = [gx[xx, at : at + pc, s].astype(F32).reshape(qr, W) for xx in range(NX)]
            rows[c][s] = jnp.concatenate(blocks, axis=1).astype(BF)
        for m in range(3):
            pre = dot(rows[c][1 if m == 2 else 0], weights[m], 1, 1)
            preb[c][:, :, m * u : (m + 1) * u] = pre.reshape(NY, yq, u).astype(BF)
        for d in SENDS:
            to = lax.rem(ym + d, NY)
            go(rc(preb[c].at[to], rs[c].at[d - 1], y_s.at[c], y_r.at[c], tp=ydev(d)))
        sent.append((rs[c], y_s.at[c]))

    def stage_e(c):
        wait_on(rs[c], y_r.at[c])

        def total(m):
            q = slice(m * u, (m + 1) * u)
            return preb[c][ym, :, q].astype(F32) + sum(rs[c][k, :, q].astype(F32) for k in range(3))

        pre_gate = total(0)
        pre_up = total(1)
        back = total(2)
        sigma = jax.nn.sigmoid(pre_gate)
        active = pre_gate * sigma
        act[c][ym, :, 0:u] = (back * pre_up * sigma * (1.0 + pre_gate * (1.0 - sigma))).astype(BF)
        act[c][ym, :, u : 2 * u] = (back * active).astype(BF)
        hid[c][ym] = (active * pre_up).astype(BF)
        own = act[c].at[ym]
        for d in SENDS:
            go(rc(own, own, a_s.at[c], a_r.at[c], tp=ydev(d)))
        sent.append((act[c].at[pl.ds(0, 3)], a_s.at[c]))

    def stage_g(c):
        qr = CHUNKS[c] * cp
        wait_on(act[c].at[pl.ds(0, 3)], a_r.at[c])
        part = dot(act[c][:, :, 0:u].reshape(qr, u), weights[0], 1, 0)
        part = part + dot(act[c][:, :, u : 2 * u].reshape(qr, u), weights[1], 1, 0)
        for xx in range(NX):
            slotp[c][xx] = part[:, xx * W : (xx + 1) * W].astype(BF)
        for d in SENDS:
            to = lax.rem(xm + d, NX)
            go(rc(slotp[c].at[to], xr[c].at[d - 1], xs_s.at[c], xs_r.at[c], tp=xdev(d)))
        sent.append((xr[c], xs_s.at[c]))

    def giveback(c, j):
        p = STARTS[c] + j
        i = lax.rem(zm + distance(c, j) + nz, nz) * 2 + lax.rem(j, 2)
        return rc(ret.at[p], retr.at[me], r_s, r_r, sp=i)

    def stage_i(c):
        at, pc = STARTS[c], CHUNKS[c]
        wait_on(xr[c], xs_r.at[c])
        slot = slotp[c][xm].astype(F32) + sum(xr[c][k].astype(F32) for k in range(3))
        ret[at : at + pc] = slot.reshape(pc, cp, W).astype(BF)
        if c == NEAR:
            retr[me] = ret[own_place]
        each_place(c, lambda j: giveback(c, j).start())

    def gwcopy(d, dst, k):
        part = pl.ds(2 * k, 2 - k)
        return rc(gs.at[lax.rem(ym + d, NY), part], gr.at[dst, part], gw_s.at[k], gw_r.at[k], tp=ydev(d))

    def weight_gradient(m, lefts):
        grad = 0.0
        for c in range(NC):
            left = lefts[c][:, :, m * u : (m + 1) * u] if m < 2 else lefts[c][...]
            grad = grad + dot(left.reshape(CHUNKS[c] * cp, u), rows[c][1 if m == 2 else 0], 0, 0)
        gs[:, m] = grad.reshape(NY, 64, yb).astype(BF)

    def gate_and_up():
        for c in range(NC):
            own = hid[c].at[ym]
            for d in SENDS:
                go(rc(own, own, hd_s.at[c], hd_r.at[c], tp=ydev(d)))
            sent.append((hid[c].at[pl.ds(0, 3)], hd_s.at[c]))
        for m in range(2):
            weight_gradient(m, act)
        for d in SENDS:
            go(gwcopy(d, ym, 0))
        sent.append((gs.at[pl.ds(0, 3), pl.ds(0, 2)], gw_s.at[0]))

    def down():
        for c in range(NC):
            wait_on(hid[c].at[pl.ds(0, 3)], hd_r.at[c])
        weight_gradient(2, hid)
        for d in SENDS:
            go(gwcopy(d, ym, 1))
        sent.append((gs.at[pl.ds(0, 3), pl.ds(2, 1)], gw_s.at[1]))
        gr[ym] = gs[ym]

    stages = (stage_a, stage_c, stage_e, stage_g, stage_i)
    for k, c in SEQUENCE:
        stages[k](c)
        if k == 3 and c == NC - 1:
            gate_and_up()
    wait_halo = rc(mhs, mh, h_s.at[0], h_r.at[0], sp=lax.rem(me + 1, ns))
    wait_halo.wait_recv()
    prev = jnp.where(me == 0, 0.0, mh[...])
    ext = jnp.concatenate([prev, mixed], axis=0)
    tap = taps_ref[...]
    conv = tap[2:3] * mixed + tap[1:2] * ext[7 : 7 + t] + tap[0:1] * ext[6 : 6 + t]
    merged = (gb_ref[...].astype(F32) * conv).astype(BF)

    wait_on(retr.at[pl.ds(0, ns - 1)], r_r)

    back_rows = retr[...].astype(F32).reshape(n_rows, W).astype(BF)
    grad_cols = ccol[...].astype(F32) + dot(pt[...], back_rows, 1, 0)
    st[tp] = grad_cols.astype(BF)

    cut = -(-t // 32) * 16
    first, rest = pl.ds(0, cut), pl.ds(cut, t - cut)

    for d in SENDS:
        go(rc(st.at[tp], st.at[tp], st_s, st_r.at[0, d], tp=ydev(d)))
        go(rc(st.at[tp], st.at[tp], st_s, st_r.at[1, d], tp=xdev(d)))
    sent.append((st.at[pl.ds(0, 6)], st_s))
    for d in SENDS:
        src = ydev(NY - d)
        wait_on(st.at[src], st_r.at[0, d])
        for e in SENDS:
            go(rc(st.at[src, first], st.at[src, first], fw_s.at[0], fw_r.at[0, e], tp=xdev(e)))
    for d in SENDS:
        src = xdev(NX - d)
        wait_on(st.at[src], st_r.at[1, d])
        for e in SENDS:
            go(rc(st.at[src, rest], st.at[src, rest], fw_s.at[1], fw_r.at[1, d], tp=ydev(e)))
    sent.append((st.at[pl.ds(0, 9), first], fw_s.at[0]))
    sent.append((st.at[pl.ds(0, 9), rest], fw_s.at[1]))

    load_o.wait()

    def pair(g):
        return rc(gpp.at[g], pr.at[g], p_s.at[g], p_r.at[g], sp=zm * 2 + 1 - core)

    def onward(z):
        return rc(gq.at[z], fr.at[zm], f_s, f_r, sp=z * 2 + core)

    def send_sums(g):
        pair(g).wait_recv()
        for far in (2, 1, 3, 0):
            yy = lax.rem(lax.div(zm, NX) + far, NY)
            z = yy * NX + lax.rem(xm + ORDER[g], NX)
            gq[z] = (gpo[g, yy] + pr[g, yy].astype(F32)).astype(BF)

            @pl.when(z != zm)
            def _(z=z):
                onward(z).start()

    for g, dx in enumerate(ORDER):
        xx = lax.rem(xm + dx, NX)
        if dx:
            wait_on(st.at[pl.ds(0, 3), first], fw_r.at[0, NX - dx])
            wait_on(st.at[pl.ds(0, 3), rest], fw_r.at[1, NX - dx])
        block = jnp.concatenate([st[yy * NX + xx] for yy in range(NY)], axis=1)
        proj = dot(block, merged, 0, 0).reshape(NY, 2, 64, W)
        proj0 = proj[:, 0]
        proj1 = proj[:, 1]
        gpo[g] = jnp.where(core == 0, proj0, proj1)
        gpp[g] = jnp.where(core == 0, proj1, proj0).astype(BF)
        pair(g).start()
        if g == 0:
            send_sums(0)
        elif g > 1:
            send_sums(g - 1)

    stream = jnp.concatenate([st[j] for j in range(NX * NY)], axis=1)
    grad_merged = dot(stream, opv[...], 1, 1)
    grad_conv = grad_merged * gb_ref[...].astype(F32)
    ghs[...] = grad_conv[0:8, :]
    halo_g = rc(ghs, gh, h_s.at[1], h_r.at[1], sp=lax.rem(me + ns - 1, ns))
    halo_g.start()
    send_sums(NX - 1)
    ggb_out[...] = (grad_merged * conv).astype(BF)
    placed[4].start()
    down()

    halo_g.wait_recv()
    following = jnp.where(me == ns - 1, 0.0, gh[...])
    extg = jnp.concatenate([grad_conv, following], axis=0)
    grad_mixed = tap[2:3] * grad_conv + tap[1:2] * extg[1 : 1 + t] + tap[0:1] * extg[2 : 2 + t]
    ggc_out[...] = (grad_mixed * ci_ref[...].astype(F32)).astype(BF)
    gci_out[...] = (grad_mixed * gc_ref[...].astype(F32)).astype(BF)
    placed[5].start()
    placed[6].start()

    for k in range(2):
        wait_on(gr.at[pl.ds(0, 3), pl.ds(2 * k, 2 - k)], gw_r.at[k])
    for m, out in enumerate((gg_out, gu_out, gd_out)):
        for yy in range(NY):
            out[:, yy * yb : (yy + 1) * yb] = gr[yy, m].astype(F32)
        placed[m].start()
    sent.append((ret.at[pl.ds(0, ns - 1)], r_s))
    sent.append((ghs, h_s.at[1]))
    for buffer, sem in sent:
        wait_on(buffer, sem)
    for g in range(NX):
        pair(g).wait_send()

    wait_on(gq.at[pl.ds(0, nz - 1)], f_s)
    wait_on(fr.at[pl.ds(0, nz - 1)], f_r)

    fr[zm] = gq[zm]
    gp_out[...] = jnp.sum(fr[...].astype(F32), axis=0)
    placed[3].start()
    for copy in placed:
        copy.wait()


def write_out(n, *refs):
    sems = refs[-1]
    copies = [pltpu.make_async_copy(refs[k], refs[n + k], sems.at[k]) for k in range(n)]
    for copy in copies:
        copy.start()
    for copy in copies:
        copy.wait()


def on_device(
    moe_input, cotangent, route_ids, route_weights, expert_gate, expert_up, expert_down,
    out_proj, gate_b, gate_c, conv_in, taps,
):
    ns = lax.axis_size("sp")
    t, model = moe_input.shape
    cap = 2 * t * route_ids.shape[1] // ns
    cp = -(-cap // 8) * 8
    n_rows = ns * cp
    yb = model // NY
    tpn = NX * NY
    units = expert_gate.shape[2]
    sds = jax.ShapeDtypeStruct
    vmem = pl.BlockSpec(memory_space=pltpu.VMEM)
    anym = pl.BlockSpec(memory_space=pltpu.HBM)
    dma = pltpu.SemaphoreType.DMA
    V = pltpu.VMEM

    def each(buffer):
        return tuple(buffer(pc * cp) for pc in CHUNKS)

    scratch = [
        V((units, model), F32), V((units, model), F32), V((units, model), F32), V((64, W), F32),
        V((t, W), BF), V((t, W), BF), V((t, W), BF), dma((7,)),
        V((2, t), jnp.int32), V((2, t), F32), V((t, W), BF), V((t, W), BF), V((t, W), BF), V((3, W), F32),
        V((t, W), BF), V((t, W), BF), V((W, model), BF), V((ns, 2, cp, W), BF), V((NX, ns, 2, cp, W), BF),
        V((NY, 3, units, yb), BF),
        each(lambda r: V((2, r, yb), BF)), each(lambda r: V((NY, r // 4, 6 * W), BF)), each(lambda r: V((3, r // 4, 6 * W), BF)),
        each(lambda r: V((NY, r // 4, 4 * W), BF)), each(lambda r: V((NY, r // 4, 2 * W), BF)), each(lambda r: V((NX, r, W), BF)),
        each(lambda r: V((3, r, W), BF)),
        V((ns, cp, W), BF), V((ns, cp, W), BF), V((t, n_rows), BF), V((tpn, t, W), BF),
        V((NY, 3, units, yb), BF), V((NY, 3, units, yb), BF), V((8, W), F32), V((8, W), F32), V((8, W), F32), V((8, W), F32),
        V((NX, NY, 64, W), F32), V((NX, NY, 64, W), BF), V((NX, NY, 64, W), BF), V((tpn, 64, W), BF), V((tpn, 64, W), BF),
        dma((9,)), dma((3,)), dma, dma, dma, dma((NC,)), dma((NC,)), dma((NC,)),
        dma((NC,)), dma((NC,)), dma((NC,)), dma((NC,)), dma((NC,)), dma((NC,)),
        dma((NC,)), dma((NC,)), dma, dma, dma, dma((2, NX)), dma((2,)), dma((2, NX)), dma((2,)), dma((2,)), dma((2,)), dma((2,)),
        dma((NX,)), dma((NX,)), dma, dma,
    ]
    out_shape = (
        sds((units, model), F32), sds((units, model), F32), sds((units, model), F32), sds((64, W), F32),
        sds((t, W), BF), sds((t, W), BF), sds((t, W), BF),
    )
    outs = pl.pallas_call(
        functools.partial(kernel, ns, cp),
        out_shape=tuple(pltpu.VMEM(o.shape, o.dtype) for o in out_shape),
        in_specs=[anym] * 12,
        out_specs=[pl.BlockSpec(memory_space=pl.ANY)] * 7,
        scratch_shapes=scratch,
        compiler_params=pltpu.CompilerParams(collective_id=0, has_side_effects=True, vmem_limit_bytes=40 * 2**20),
    )(
        *(
            pltpu.with_memory_space_constraint(a, pltpu.HBM)
            for a in (
                route_ids.T, route_weights.T, moe_input, cotangent, expert_gate[0].T, expert_up[0].T, expert_down[0],
                out_proj, gate_b, gate_c, conv_in, taps,
            )
        )
    )
    outs = pl.pallas_call(
        functools.partial(write_out, 7),
        out_shape=tuple(pltpu.HBM(o.shape, o.dtype) for o in out_shape),
        in_specs=[vmem] * 7,
        out_specs=[anym] * 7,
        scratch_shapes=[dma((7,))],
    )(*(pltpu.with_memory_space_constraint(o, pltpu.VMEM) for o in outs))
    gg, gu, gd, gp, ggb, ggc, gci = outs
    return gg.T[None], gu.T[None], gd[None], gp.T, ggb, ggc, gci


def solution(mesh):
    row, cols = P("sp", None), P("sp", "tp")
    return jax.shard_map(
        on_device,
        mesh=mesh,
        in_specs=(
            row, row, row, row, P("sp", None, "tp"), P("sp", None, "tp"), P("sp", "tp", None), P("tp", None),
            cols, cols, cols, P(None, "tp"),
        ),
        out_specs=(
            P("sp", None, "tp"), P("sp", None, "tp"), P("sp", "tp", None), P("tp", "sp"), cols, cols, cols,
        ),
        check_vma=False,
    )
```

```python
import functools

import jax
import jax.numpy as jnp
from jax import lax
from jax.experimental import pallas as pl
from jax.experimental.pallas import tpu as pltpu
from jax.sharding import PartitionSpec as P

MESH = pl.DeviceIdType.MESH
BF = jnp.bfloat16
F32 = jnp.float32
NX = 4
NY = 4
W = 128


def dot(a, b, ca, cb):
    return lax.dot_general(a, b, (((ca,), (cb,)), ((), ())), preferred_element_type=F32)


CHUNKS = (8, 8, 8, 8)
RANGES = (0, 3, 2, 1)
NEAR = RANGES.index(0)
STARTS = tuple(sum(CHUNKS[:k]) for k in range(len(CHUNKS)))
NC = len(CHUNKS)
SEQUENCE = (
    (0, 0), (1, 0), (0, 1), (2, 0), (0, 2), (1, 1), (0, 3), (3, 0), (1, 2), (2, 1),
    (1, 3), (3, 1), (2, 2), (4, 0), (2, 3), (3, 2), (4, 1), (3, 3), (4, 2), (4, 3),
)
ORDER = (0, 1, 3, 2)
SENDS = (2, 1, 3)


def kernel(
    ns, cp,
    ids_hbm, wts_hbm, x_hbm, c_hbm, wg_hbm, wu_hbm, wd_hbm, op_hbm, gb_hbm, gc_hbm, ci_hbm, taps_hbm,
    gg_any, gu_any, gd_any, gp_any, ggb_any, ggc_any, gci_any,
    gg_out, gu_out, gd_out, gp_out, ggb_out, ggc_out, gci_out, out_sem,
    ids_ref, wts_ref, gb_ref, gc_ref, ci_ref, taps_ref,
    xcol, ccol, opv, disp, gx, wx, rows, preb, rs, act, hid, slotp, xr, ret, retr, pt, st,
    gs, gr, mhs, mh, ghs, gh, gpo, gpp, pr, gq, fr,
    loc_sem, bsem_w, wsem_s, wsem_r, d_s, d_r, gx_s, gx_r, y_s, y_r, a_s, a_r, hd_s, hd_r,
    xs_s, xs_r, r_s, r_r, st_s, st_r, fw_s, fw_r, gw_s, gw_r, h_s, h_r, p_s, p_r, f_s, f_r,
):
    me = lax.axis_index("sp")
    tp = lax.axis_index("tp")
    ym = lax.div(tp, NX)
    xm = lax.rem(tp, NX)
    core = lax.rem(me, 2)
    zm = lax.div(me, 2)
    nz = ns // 2
    t = ids_ref.shape[1]
    n_rows = ns * cp
    u = 2 * W
    yb = 4 * W

    def xdev(d):
        return ym * NX + lax.rem(xm + d, NX)

    def ydev(d):
        return lax.rem(ym + d, NY) * NX + xm

    def rc(src, dst, ss, rs, **where):
        return pltpu.make_async_remote_copy(
            src_ref=src, dst_ref=dst, send_sem=ss, recv_sem=rs, device_id=where, device_id_type=MESH
        )

    def offset(k):
        return lax.div(k + 1, 2) * (2 * lax.rem(k, 2) - 1)

    placed = [
        pltpu.make_async_copy(src, dst, out_sem.at[k])
        for k, (src, dst) in enumerate(
            (
                (gg_out, gg_any), (gu_out, gu_any), (gd_out, gd_any), (gp_out, gp_any), (ggb_out, ggb_any),
                (ggc_out, ggc_any), (gci_out, gci_any),
            )
        )
    ]

    def wait_on(buffer, sem):
        rc(buffer, buffer, sem, sem, tp=lax.rem(tp + 1, NX * NY)).wait_recv()

    sent = []

    def go(copy):
        copy.start()

    barrier = pltpu.get_barrier_semaphore()
    small = [
        pltpu.make_async_copy(src, dst, loc_sem.at[k])
        for k, (src, dst) in enumerate(
            (
                (ids_hbm, ids_ref), (wts_hbm, wts_ref), (gb_hbm, gb_ref), (gc_hbm, gc_ref), (ci_hbm, ci_ref),
                (taps_hbm, taps_ref),
            )
        )
    ]
    cols = pl.ds(pl.multiple_of(tp * W, W), W)
    load_x = pltpu.make_async_copy(x_hbm.at[:, cols], xcol, loc_sem.at[6])
    load_c = pltpu.make_async_copy(c_hbm.at[:, cols], ccol, loc_sem.at[7])
    load_o = pltpu.make_async_copy(op_hbm, opv, loc_sem.at[8])
    mats = (wg_hbm, wu_hbm, wd_hbm)
    ycols = pl.ds(pl.multiple_of(ym * yb, yb), yb)
    load_w = [pltpu.make_async_copy(mats[m].at[:, ycols], wx.at[ym, m], bsem_w.at[m]) for m in range(3)]
    small[0].start()

    @pl.loop(1, ns)
    def _(d):
        pl.semaphore_signal(barrier, inc=1, device_id={"sp": lax.rem(me + d, ns)}, device_id_type=MESH)

    @pl.loop(1, NX * NY)
    def _(d):
        pl.semaphore_signal(barrier, inc=1, device_id={"tp": lax.rem(tp + d, NX * NY)}, device_id_type=MESH)

    small[1].start()
    load_x.start()
    load_c.start()
    for copy in small[2:]:
        copy.start()
    for copy in load_w:
        copy.start()
    load_o.start()

    small[0].wait()
    small[1].wait()
    id0 = ids_ref[0:1, :]
    id1 = ids_ref[1:2, :]
    eio = lax.broadcasted_iota(jnp.int32, (ns, t), 0)
    oh0 = (eio == id0).astype(F32)
    oh1 = (eio == id1).astype(F32)
    before = (lax.broadcasted_iota(jnp.int32, (t, t), 0) < lax.broadcasted_iota(jnp.int32, (t, t), 1)).astype(F32).astype(BF)
    cum = dot((oh0 + oh1).astype(BF), before, 1, 0)
    slot0 = id0 * cp + jnp.sum(oh0 * cum, axis=0, keepdims=True).astype(jnp.int32)
    slot1 = id1 * cp + jnp.sum(oh1 * cum, axis=0, keepdims=True).astype(jnp.int32)
    rio = lax.broadcasted_iota(jnp.int32, (n_rows, t), 0)
    p0 = rio == slot0
    p1 = rio == slot1
    pmat = jnp.where(p0 | p1, 1.0, 0.0)
    wslot = jnp.sum(jnp.where(p0, wts_ref[0:1, :], jnp.where(p1, wts_ref[1:2, :], 0.0)), axis=1, keepdims=True)
    pb = pmat.astype(BF)
    load_x.wait()
    load_c.wait()
    picked = dot(pb, jnp.concatenate([xcol[...], ccol[...]], axis=1), 1, 0)
    disp[:, 0] = picked[:, :W].reshape(ns, cp, W).astype(BF)
    disp[:, 1] = (wslot * picked[:, W:]).reshape(ns, cp, W).astype(BF)

    for copy in small[2:]:
        copy.wait()
    mixed = gc_ref[...].astype(F32) * ci_ref[...].astype(F32)
    mhs[...] = mixed[t - 8 :, :]

    pl.semaphore_wait(barrier, ns - 1 + NX * NY - 1)

    def distance(c, j):
        return offset(RANGES[c] * 4 + lax.div(j, 2))

    def dispatch(c, j):
        i = lax.rem(zm - distance(c, j) + nz, nz) * 2 + lax.rem(j, 2)
        place = STARTS[c] + j - lax.rem(j, 2) + core
        return rc(disp.at[i], gx.at[xm, place], d_s, d_r.at[c], sp=i)

    def each_place(c, act_on):
        if c == NEAR:
            act_on(1 - core)

        @pl.loop(2 if c == NEAR else 0, CHUNKS[c])
        def _(j):
            act_on(j)

    own_place = STARTS[NEAR] + core
    for c in range(NC):
        each_place(c, lambda j, c=c: dispatch(c, j).start())

    def wcopy(d, m, dst):
        block = pl.ds(pl.multiple_of(lax.rem(ym + d, NY) * yb, yb), yb)
        return rc(mats[m].at[:, block], wx.at[dst, m], wsem_s, wsem_r, tp=ydev(d))

    for d in (1, 3, 2):
        for m in range(3):
            go(wcopy(d, m, ym))

    sent.append((wx.at[pl.ds(0, 3)], wsem_s))
    halo_m = rc(mhs, mh, h_s.at[0], h_r.at[0], sp=lax.rem(me + 1, ns))
    halo_m.start()
    sent.append((mhs, h_s.at[0]))
    sent.append((disp.at[pl.ds(0, ns - 1)], d_s))

    gx[xm, own_place] = disp[me]

    pt[...] = pmat.T.astype(BF)

    weights = []

    def stage_a(c):
        at, pc = STARTS[c], CHUNKS[c]
        wait_on(gx.at[xm, pl.ds(at, pc - (c == NEAR))], d_r.at[c])
        part = gx.at[xm, pl.ds(at, pc)]
        for d in SENDS:
            go(rc(part, part, gx_s.at[c], gx_r.at[c], tp=xdev(d)))
        sent.append((gx.at[pl.ds(0, 3), pl.ds(at, pc)], gx_s.at[c]))

    def stage_c(c):
        at, pc = STARTS[c], CHUNKS[c]
        qr = pc * cp
        yq = qr // NY
        if c == 0:
            for m in range(3):
                load_w[m].wait()
            wait_on(wx.at[pl.ds(0, 3)], wsem_r)
            weights.extend(jnp.concatenate([wx[yy, m] for yy in range(NY)], axis=0) for m in range(3))
        wait_on(gx.at[pl.ds(0, 3), pl.ds(at, pc)], gx_r.at[c])
        for s in range(2):
            blocks = [gx[xx, at : at + pc, s].astype(F32).reshape(qr, W) for xx in range(NX)]
            rows[c][s] = jnp.concatenate(blocks, axis=1).astype(BF)
        for m in range(3):
            pre = dot(rows[c][1 if m == 2 else 0], weights[m], 1, 1)
            preb[c][:, :, m * u : (m + 1) * u] = pre.reshape(NY, yq, u).astype(BF)
        for d in SENDS:
            to = lax.rem(ym + d, NY)
            go(rc(preb[c].at[to], rs[c].at[d - 1], y_s.at[c], y_r.at[c], tp=ydev(d)))
        sent.append((rs[c], y_s.at[c]))

    def stage_e(c):
        wait_on(rs[c], y_r.at[c])

        def total(m):
            q = slice(m * u, (m + 1) * u)
            return preb[c][ym, :, q].astype(F32) + sum(rs[c][k, :, q].astype(F32) for k in range(3))

        pre_gate = total(0)
        pre_up = total(1)
        back = total(2)
        sigma = jax.nn.sigmoid(pre_gate)
        active = pre_gate * sigma
        act[c][ym, :, 0:u] = (back * pre_up * sigma * (1.0 + pre_gate * (1.0 - sigma))).astype(BF)
        act[c][ym, :, u : 2 * u] = (back * active).astype(BF)
        hid[c][ym] = (active * pre_up).astype(BF)
        own = act[c].at[ym]
        for d in SENDS:
            go(rc(own, own, a_s.at[c], a_r.at[c], tp=ydev(d)))
        sent.append((act[c].at[pl.ds(0, 3)], a_s.at[c]))

    def stage_g(c):
        qr = CHUNKS[c] * cp
        wait_on(act[c].at[pl.ds(0, 3)], a_r.at[c])
        part = dot(act[c][:, :, 0:u].reshape(qr, u), weights[0], 1, 0)
        part = part + dot(act[c][:, :, u : 2 * u].reshape(qr, u), weights[1], 1, 0)
        for xx in range(NX):
            slotp[c][xx] = part[:, xx * W : (xx + 1) * W].astype(BF)
        for d in SENDS:
            to = lax.rem(xm + d, NX)
            go(rc(slotp[c].at[to], xr[c].at[d - 1], xs_s.at[c], xs_r.at[c], tp=xdev(d)))
        sent.append((xr[c], xs_s.at[c]))

    def giveback(c, j):
        p = STARTS[c] + j
        i = lax.rem(zm + distance(c, j) + nz, nz) * 2 + lax.rem(j, 2)
        return rc(ret.at[p], retr.at[me], r_s, r_r, sp=i)

    def stage_i(c):
        at, pc = STARTS[c], CHUNKS[c]
        wait_on(xr[c], xs_r.at[c])
        slot = slotp[c][xm].astype(F32) + sum(xr[c][k].astype(F32) for k in range(3))
        ret[at : at + pc] = slot.reshape(pc, cp, W).astype(BF)
        if c == NEAR:
            retr[me] = ret[own_place]
        each_place(c, lambda j: giveback(c, j).start())

    def gwcopy(d, dst, k):
        part = pl.ds(2 * k, 2 - k)
        return rc(gs.at[lax.rem(ym + d, NY), part], gr.at[dst, part], gw_s.at[k], gw_r.at[k], tp=ydev(d))

    def weight_gradient(m, lefts):
        grad = 0.0
        for c in range(NC):
            left = lefts[c][:, :, m * u : (m + 1) * u] if m < 2 else lefts[c][...]
            grad = grad + dot(left.reshape(CHUNKS[c] * cp, u), rows[c][1 if m == 2 else 0], 0, 0)
        gs[:, m] = grad.reshape(NY, 64, yb).astype(BF)

    def gate_and_up():
        for c in range(NC):
            own = hid[c].at[ym]
            for d in SENDS:
                go(rc(own, own, hd_s.at[c], hd_r.at[c], tp=ydev(d)))
            sent.append((hid[c].at[pl.ds(0, 3)], hd_s.at[c]))
        for m in range(2):
            weight_gradient(m, act)
        for d in SENDS:
            go(gwcopy(d, ym, 0))
        sent.append((gs.at[pl.ds(0, 3), pl.ds(0, 2)], gw_s.at[0]))

    def down():
        for c in range(NC):
            wait_on(hid[c].at[pl.ds(0, 3)], hd_r.at[c])
        weight_gradient(2, hid)
        for d in SENDS:
            go(gwcopy(d, ym, 1))
        sent.append((gs.at[pl.ds(0, 3), pl.ds(2, 1)], gw_s.at[1]))
        gr[ym] = gs[ym]

    stages = (stage_a, stage_c, stage_e, stage_g, stage_i)
    for k, c in SEQUENCE:
        stages[k](c)
        if k == 3 and c == NC - 1:
            gate_and_up()
    wait_halo = rc(mhs, mh, h_s.at[0], h_r.at[0], sp=lax.rem(me + 1, ns))
    wait_halo.wait_recv()
    prev = jnp.where(me == 0, 0.0, mh[...])
    ext = jnp.concatenate([prev, mixed], axis=0)
    tap = taps_ref[...]
    conv = tap[2:3] * mixed + tap[1:2] * ext[7 : 7 + t] + tap[0:1] * ext[6 : 6 + t]
    merged = (gb_ref[...].astype(F32) * conv).astype(BF)

    wait_on(retr.at[pl.ds(0, ns - 1)], r_r)

    back_rows = retr[...].astype(F32).reshape(n_rows, W).astype(BF)
    grad_cols = ccol[...].astype(F32) + dot(pt[...], back_rows, 1, 0)
    st[tp] = grad_cols.astype(BF)

    cut = -(-t // 32) * 16
    first, rest = pl.ds(0, cut), pl.ds(cut, t - cut)

    for d in SENDS:
        go(rc(st.at[tp], st.at[tp], st_s, st_r.at[0, d], tp=ydev(d)))
        go(rc(st.at[tp], st.at[tp], st_s, st_r.at[1, d], tp=xdev(d)))
    sent.append((st.at[pl.ds(0, 6)], st_s))
    for d in (1, 3, 2):
        src = ydev(NY - d)
        wait_on(st.at[src], st_r.at[0, d])
        for e in SENDS:
            go(rc(st.at[src, first], st.at[src, first], fw_s.at[0], fw_r.at[0, e], tp=xdev(e)))

    load_o.wait()

    def forward_x():
        for d in (1, 3, 2):
            src = xdev(NX - d)
            wait_on(st.at[src], st_r.at[1, d])
            for e in SENDS:
                go(rc(st.at[src, rest], st.at[src, rest], fw_s.at[1], fw_r.at[1, d], tp=ydev(e)))
        sent.append((st.at[pl.ds(0, 9), first], fw_s.at[0]))
        sent.append((st.at[pl.ds(0, 9), rest], fw_s.at[1]))

    def pair(g):
        return rc(gpp.at[g], pr.at[g], p_s.at[g], p_r.at[g], sp=zm * 2 + 1 - core)

    def onward(z):
        return rc(gq.at[z], fr.at[zm], f_s, f_r, sp=z * 2 + core)

    def send_sums(g):
        pair(g).wait_recv()
        for far in (2, 1, 3, 0):
            yy = lax.rem(lax.div(zm, NX) + far, NY)
            z = yy * NX + lax.rem(xm + ORDER[g], NX)
            gq[z] = (gpo[g, yy] + pr[g, yy].astype(F32)).astype(BF)

            @pl.when(z != zm)
            def _(z=z):
                onward(z).start()

    for g, dx in enumerate(ORDER):
        xx = lax.rem(xm + dx, NX)
        if dx:
            wait_on(st.at[pl.ds(0, 3), first], fw_r.at[0, NX - dx])
            wait_on(st.at[pl.ds(0, 3), rest], fw_r.at[1, NX - dx])
        block = jnp.concatenate([st[yy * NX + xx] for yy in range(NY)], axis=1)
        proj = dot(block, merged, 0, 0).reshape(NY, 2, 64, W)
        proj0 = proj[:, 0]
        proj1 = proj[:, 1]
        gpo[g] = jnp.where(core == 0, proj0, proj1)
        gpp[g] = jnp.where(core == 0, proj1, proj0).astype(BF)
        pair(g).start()
        if g == 0:
            forward_x()
            send_sums(0)
        elif g > 1:
            send_sums(g - 1)

    stream = jnp.concatenate([st[j] for j in range(NX * NY)], axis=1)
    grad_merged = dot(stream, opv[...], 1, 1)
    grad_conv = grad_merged * gb_ref[...].astype(F32)
    ghs[...] = grad_conv[0:8, :]
    halo_g = rc(ghs, gh, h_s.at[1], h_r.at[1], sp=lax.rem(me + ns - 1, ns))
    halo_g.start()
    send_sums(NX - 1)
    ggb_out[...] = (grad_merged * conv).astype(BF)
    placed[4].start()
    down()

    halo_g.wait_recv()
    following = jnp.where(me == ns - 1, 0.0, gh[...])
    extg = jnp.concatenate([grad_conv, following], axis=0)
    grad_mixed = tap[2:3] * grad_conv + tap[1:2] * extg[1 : 1 + t] + tap[0:1] * extg[2 : 2 + t]
    ggc_out[...] = (grad_mixed * ci_ref[...].astype(F32)).astype(BF)
    gci_out[...] = (grad_mixed * gc_ref[...].astype(F32)).astype(BF)
    placed[5].start()
    placed[6].start()

    for k in range(2):
        wait_on(gr.at[pl.ds(0, 3), pl.ds(2 * k, 2 - k)], gw_r.at[k])
    for m, out in enumerate((gg_out, gu_out, gd_out)):
        for yy in range(NY):
            out[:, yy * yb : (yy + 1) * yb] = gr[yy, m].astype(F32)
        placed[m].start()
    sent.append((ret.at[pl.ds(0, ns - 1)], r_s))
    sent.append((ghs, h_s.at[1]))
    for buffer, sem in sent:
        wait_on(buffer, sem)
    for g in range(NX):
        pair(g).wait_send()

    wait_on(gq.at[pl.ds(0, nz - 1)], f_s)
    wait_on(fr.at[pl.ds(0, nz - 1)], f_r)

    fr[zm] = gq[zm]
    gp_out[...] = jnp.sum(fr[...].astype(F32), axis=0)
    placed[3].start()
    for copy in placed:
        copy.wait()


def write_out(n, *refs):
    sems = refs[-1]
    copies = [pltpu.make_async_copy(refs[k], refs[n + k], sems.at[k]) for k in range(n)]
    for copy in copies:
        copy.start()
    for copy in copies:
        copy.wait()


def on_device(
    moe_input, cotangent, route_ids, route_weights, expert_gate, expert_up, expert_down,
    out_proj, gate_b, gate_c, conv_in, taps,
):
    ns = lax.axis_size("sp")
    t, model = moe_input.shape
    cap = 2 * t * route_ids.shape[1] // ns
    cp = -(-cap // 8) * 8
    n_rows = ns * cp
    yb = model // NY
    tpn = NX * NY
    units = expert_gate.shape[2]
    sds = jax.ShapeDtypeStruct
    vmem = pl.BlockSpec(memory_space=pltpu.VMEM)
    anym = pl.BlockSpec(memory_space=pltpu.HBM)
    dma = pltpu.SemaphoreType.DMA
    V = pltpu.VMEM

    def each(buffer):
        return tuple(buffer(pc * cp) for pc in CHUNKS)

    scratch = [
        V((units, model), F32), V((units, model), F32), V((units, model), F32), V((64, W), F32),
        V((t, W), BF), V((t, W), BF), V((t, W), BF), dma((7,)),
        V((2, t), jnp.int32), V((2, t), F32), V((t, W), BF), V((t, W), BF), V((t, W), BF), V((3, W), F32),
        V((t, W), BF), V((t, W), BF), V((W, model), BF), V((ns, 2, cp, W), BF), V((NX, ns, 2, cp, W), BF),
        V((NY, 3, units, yb), BF),
        each(lambda r: V((2, r, yb), BF)), each(lambda r: V((NY, r // 4, 6 * W), BF)), each(lambda r: V((3, r // 4, 6 * W), BF)),
        each(lambda r: V((NY, r // 4, 4 * W), BF)), each(lambda r: V((NY, r // 4, 2 * W), BF)), each(lambda r: V((NX, r, W), BF)),
        each(lambda r: V((3, r, W), BF)),
        V((ns, cp, W), BF), V((ns, cp, W), BF), V((t, n_rows), BF), V((tpn, t, W), BF),
        V((NY, 3, units, yb), BF), V((NY, 3, units, yb), BF), V((8, W), F32), V((8, W), F32), V((8, W), F32), V((8, W), F32),
        V((NX, NY, 64, W), F32), V((NX, NY, 64, W), BF), V((NX, NY, 64, W), BF), V((tpn, 64, W), BF), V((tpn, 64, W), BF),
        dma((9,)), dma((3,)), dma, dma, dma, dma((NC,)), dma((NC,)), dma((NC,)),
        dma((NC,)), dma((NC,)), dma((NC,)), dma((NC,)), dma((NC,)), dma((NC,)),
        dma((NC,)), dma((NC,)), dma, dma, dma, dma((2, NX)), dma((2,)), dma((2, NX)), dma((2,)), dma((2,)), dma((2,)), dma((2,)),
        dma((NX,)), dma((NX,)), dma, dma,
    ]
    out_shape = (
        sds((units, model), F32), sds((units, model), F32), sds((units, model), F32), sds((64, W), F32),
        sds((t, W), BF), sds((t, W), BF), sds((t, W), BF),
    )
    outs = pl.pallas_call(
        functools.partial(kernel, ns, cp),
        out_shape=tuple(pltpu.VMEM(o.shape, o.dtype) for o in out_shape),
        in_specs=[anym] * 12,
        out_specs=[pl.BlockSpec(memory_space=pl.ANY)] * 7,
        scratch_shapes=scratch,
        compiler_params=pltpu.CompilerParams(collective_id=0, has_side_effects=True, vmem_limit_bytes=40 * 2**20),
    )(
        *(
            pltpu.with_memory_space_constraint(a, pltpu.HBM)
            for a in (
                route_ids.T, route_weights.T, moe_input, cotangent, expert_gate[0].T, expert_up[0].T, expert_down[0],
                out_proj, gate_b, gate_c, conv_in, taps,
            )
        )
    )
    outs = pl.pallas_call(
        functools.partial(write_out, 7),
        out_shape=tuple(pltpu.HBM(o.shape, o.dtype) for o in out_shape),
        in_specs=[vmem] * 7,
        out_specs=[anym] * 7,
        scratch_shapes=[dma((7,))],
    )(*(pltpu.with_memory_space_constraint(o, pltpu.VMEM) for o in outs))
    gg, gu, gd, gp, ggb, ggc, gci = outs
    return gg.T[None], gu.T[None], gd[None], gp.T, ggb, ggc, gci


def solution(mesh):
    row, cols = P("sp", None), P("sp", "tp")
    return jax.shard_map(
        on_device,
        mesh=mesh,
        in_specs=(
            row, row, row, row, P("sp", None, "tp"), P("sp", None, "tp"), P("sp", "tp", None), P("tp", None),
            cols, cols, cols, P(None, "tp"),
        ),
        out_specs=(
            P("sp", None, "tp"), P("sp", None, "tp"), P("sp", "tp", None), P("tp", "sp"), cols, cols, cols,
        ),
        check_vma=False,
    )
```
